512 devices in a mesh: sp: 32 (over z, core), tp: 16 (over y, x).
Axes of the slice: x: 4, y: 4, z: 16, core: 2. Of those that a mesh axis runs over, the one named last changes fastest.
Arguments:
- stream: bfloat16 [12288, 2048], P('sp', 'tp'), may hold values from -6 to 6
- doc_ids: int32 [12288], P('sp'), may hold values from 0 to 9, never falling along the last dimension, each value on 1 to 2304 neighbouring positions
- w_value: bfloat16 [3, 2048, 2048], P(None, None, 'tp'), may hold values from -0.125 to 0.125
- w_gate: bfloat16 [3, 2048, 2048], P(None, None, 'tp'), may hold values from -0.125 to 0.125
- conv_kernel: bfloat16 [3, 31, 2048], P(None, None, 'tp'), may hold values from -4 to 4
- conv_gain: float32 [3, 2048], replicated, may hold values from 0.1 to 1.9
- conv_shift: float32 [3, 2048], replicated, may hold values from -3 to 3
- w_proj: bfloat16 [3, 2048, 2048], P(None, None, 'tp'), may hold values from -0.125 to 0.125
- out_gain: float32 [3, 2048], replicated, may hold values from 0.1 to 1.9
- out_shift: float32 [3, 2048], replicated, may hold values from -3 to 3
Outputs:
- result: bfloat16 [12288, 2048], P('sp', 'tp')
The draws below stay inside these ranges and needn't reach their ends.
All inputs are finite; a program needn't handle non-finite values.
Results may differ from the reference program's by a relative error of at most 0.013.
Values may be sent and summed in bfloat16 or wider, within the bound.
A program may use at most 64 MiB of HBM per device.

```python
import math
import jax
import jax.numpy as jnp
import numpy as np
from jax import lax

D = 2048
DC = 2048
KERNEL = 31
LAYERS = 3
TOK_DEV = 384
HALF = 15
TOKENS = 12288


def draw_conv_kernel(key, part):
    first = jax.random.fold_in(key, 11)
    second = jax.random.fold_in(key, 12)
    rough = jax.random.uniform(second, (DC,), jnp.float32, 0.5, 1.5)
    base = jnp.clip(jax.random.normal(first, (LAYERS, KERNEL, DC), jnp.float32), -4.0, 4.0)
    ramp = jnp.exp(jnp.linspace(math.log(0.4), math.log(2.0), DC))
    return (base * (ramp * rough)[None, None, :] * KERNEL ** (-0.5)).astype(jnp.bfloat16)


def steps_of(rng, shape, pieces, smallest, largest):
    def one(axis_at, shards_of):
        steps = jax.random.uniform(jax.random.fold_in(jax.random.fold_in(rng, 6), axis_at), (shards_of,), jnp.float32, smallest / len(pieces), largest / len(pieces))
        return jnp.repeat(jnp.exp(steps), shape[axis_at] // shards_of).reshape((-1,) + (1,) * (len(shape) - axis_at - 1))

    level = one(*pieces[0])
    for cut in pieces[1:]:
        level = level * one(*cut)
    return level


def split_up(count, total, reach, slope):
    loads = [(1 << 20) // math.isqrt(grade ** slope) + 1 for grade in range(2, count + 1)]
    surplus, counts = total - reach - (count - 1), [1] * (count - 1)
    while surplus > 0:
        free = [i for i in range(count - 1) if counts[i] < reach]
        pool, left = sum([loads[i] for i in free]), surplus
        for i in free:
            more = min(reach - counts[i], max(1, left * loads[i] // pool), surplus)
            counts[i] = counts[i] + more
            surplus = surplus - more
    return np.array([reach] + counts)


def ragged(key, amount, total, limit, lean):
    if amount == 2:
        one = jax.random.randint(key, (), max(1, total - limit), min(limit, total - 1) + 1)
        return jnp.stack([one, total - one])
    lengths = jnp.asarray(split_up(amount, total, limit, lean), jnp.int32)
    twos = (amount - 1) // 2
    donor, sink = lengths[1:1 + 2 * twos:2], lengths[2:2 + 2 * twos:2]
    slack = jnp.minimum(donor - 1, limit - sink)
    passed = jax.random.randint(jax.random.fold_in(key, 1), (twos,), 0, 1 << 20) % (slack + 1)
    lengths = lengths.at[1:1 + 2 * twos:2].set(donor - passed).at[2:2 + 2 * twos:2].set(sink + passed)
    return lengths[jax.random.permutation(jax.random.fold_in(key, 2), amount)]


def bell_draw(own_key, extent, scale, limit, shards=(), held_as=jnp.bfloat16):
    level = steps_of(own_key, extent, shards, -0.22, 0.18) if shards else 1.0
    drawn = jax.random.normal(own_key, extent, jnp.float32) * scale * level
    return jnp.minimum(jnp.maximum(drawn, -limit), limit).astype(held_as)


def setup_inputs(seed: int = 0) -> dict:
    arg_keys = jax.random.split(jax.random.key(seed), 11)
    stream = bell_draw(arg_keys[0], (TOKENS, D), 1.0, 6.0, ((0, 32), (1, 16)))
    doc_ids = jnp.searchsorted(jnp.cumsum(ragged(arg_keys[1], TOKENS // (3 * TOK_DEV), TOKENS, 6 * TOK_DEV, 2)), jnp.arange(TOKENS), side="right").astype(jnp.int32)
    w_value = bell_draw(arg_keys[2], (LAYERS, D, DC), D ** -0.5, 0.125, ((2, 16),))
    w_gate = bell_draw(arg_keys[3], (LAYERS, D, DC), D ** -0.5, 0.125, ((2, 16),))
    conv_kernel = draw_conv_kernel(jax.random.fold_in(arg_keys[10], 71), 0)
    conv_gain = jnp.clip(1.0 + 0.18 * jax.random.normal(arg_keys[5], (LAYERS, DC), jnp.float32), 0.1, 1.9)
    conv_shift = bell_draw(arg_keys[6], (LAYERS, DC), 0.5, 3.0, (), jnp.float32)
    w_proj = bell_draw(arg_keys[7], (LAYERS, DC, D), DC ** -0.5, 0.125, ((2, 16),))
    out_gain = jnp.clip(1.0 + 0.18 * jax.random.normal(arg_keys[8], (LAYERS, D), jnp.float32), 0.1, 1.9)
    out_shift = bell_draw(arg_keys[9], (LAYERS, D), 0.5, 3.0, (), jnp.float32)
    return dict(stream=stream, doc_ids=doc_ids, w_value=w_value, w_gate=w_gate, conv_kernel=conv_kernel, conv_gain=conv_gain, conv_shift=conv_shift, w_proj=w_proj, out_gain=out_gain, out_shift=out_shift)


ALPHA = 2.0 ** 0.25
EPS = 1e-05

def reference(stream, doc_ids, w_value, w_gate, conv_kernel, conv_gain, conv_shift, w_proj, out_gain, out_shift):
    hidden = stream
    seg_pad = jnp.pad(doc_ids, (HALF, HALF), constant_values=-1)
    for layer in range(LAYERS):
        lin = jnp.dot(hidden, w_value[layer], preferred_element_type=jnp.float32)
        gat = jnp.dot(hidden, w_gate[layer], preferred_element_type=jnp.float32)
        glu = (lin * jax.nn.sigmoid(gat)).astype(jnp.bfloat16)
        padded = jnp.pad(glu.astype(jnp.float32), ((HALF, HALF), (0, 0)))
        taps = conv_kernel[layer].astype(jnp.float32)
        total = jnp.zeros((TOKENS, DC), jnp.float32)
        for k in range(KERNEL):
            keep = (seg_pad[k:k + TOKENS] == doc_ids).astype(jnp.float32)[:, None]
            total = total + padded[k:k + TOKENS] * keep * taps[k][None, :]
        conv = total.astype(jnp.bfloat16).astype(jnp.float32)
        centre = lax.optimization_barrier(jnp.mean(conv, axis=1, keepdims=True))
        spread = lax.optimization_barrier(jnp.mean(jnp.square(conv - centre), axis=1, keepdims=True))
        normed = (conv - centre) * jax.lax.rsqrt(spread + EPS) * conv_gain[layer] + conv_shift[layer]
        act = jax.nn.silu(normed).astype(jnp.bfloat16)
        mixed = ALPHA * hidden.astype(jnp.float32) + jnp.dot(act, w_proj[layer], preferred_element_type=jnp.float32)
        mean_z = lax.optimization_barrier(jnp.mean(mixed, axis=1, keepdims=True))
        var_z = lax.optimization_barrier(jnp.mean(jnp.square(mixed - mean_z), axis=1, keepdims=True))
        hidden = ((mixed - mean_z) * jax.lax.rsqrt(var_z + EPS) * out_gain[layer] + out_shift[layer]).astype(jnp.bfloat16)
    return hidden
```

```python
import functools

import jax
import jax.numpy as jnp
from jax import lax
from jax.experimental import pallas as pl
from jax.experimental.pallas import tpu as pltpu
from jax.sharding import PartitionSpec as P

LAYERS = 3
KERNEL = 31
HALF = 15
PAD = 16
LANES = 128
SIDE = 4
PEERS = SIDE * SIDE
ALPHA = 2.0**0.25
EPS = 1e-05
MESH = pl.DeviceIdType.MESH


class Tree:
    def __init__(self, env, gather, piece, row0, rows, x_first, up):
        self.env, self.g, self.p = env, gather, piece
        self.row0, self.rows, self.x_first, self.up = row0, rows, x_first, up

    def block(self, du, dv):
        dx, dy = (du, dv) if self.x_first else (dv, du)
        e = self.env
        slot = lax.rem(e["y"] + dy + SIDE, SIDE) * SIDE + lax.rem(e["x"] + dx + SIDE, SIDE)
        return e["gbuf"].at[self.g, slot, pl.ds(self.row0, self.rows), :]

    def copy(self, du, dv, eu, ev):
        e = self.env
        ex, ey = (eu, ev) if self.x_first else (ev, eu)
        peer = lax.rem(e["y"] + ey + SIDE, SIDE) * SIDE + lax.rem(e["x"] + ex + SIDE, SIDE)
        there = ((du - eu) % SIDE) * SIDE + (dv - ev) % SIDE
        ref = self.block(du, dv)
        return pltpu.make_async_remote_copy(
            src_ref=ref,
            dst_ref=ref,
            send_sem=e["send"].at[self.g, self.p, there],
            recv_sem=e["recv"].at[self.g, self.p, there],
            device_id=(e["s"], peer),
            device_id_type=MESH,
        )

    def sends(self):
        up = 1 if self.up else -1
        out = {(0, 0): [(1, 0), (-1, 0), (0, 1), (0, -1)]}
        for du in (-1, 1, 2):
            out[(du, 0)] = [(0, 1), (0, -1)]
        out[(-up, 0)].insert(0, (up, 0))
        for du in (0, 1, -1, 2):
            forward = up if du in (0, 2) else -up
            out[(du, -forward)] = [(0, forward)]
        return out

    def order(self):
        first = [(-1, 0), (1, 0)] if self.up else [(1, 0), (-1, 0)]
        return first + [(0, -1), (0, 1), (2, 0), (-1, -1), (-1, 1), (1, -1), (1, 1), (2, -1), (2, 1)] + [
            (0, 2), (-1, 2), (1, 2), (2, 2)
        ]

    def start(self):
        for eu, ev in self.sends()[(0, 0)]:
            self.copy(0, 0, eu, ev).start()

    def arrive(self, du, dv):
        index = (du % SIDE) * SIDE + dv % SIDE
        e = self.env
        ref = self.block(du, dv)
        pltpu.make_async_remote_copy(
            src_ref=ref,
            dst_ref=ref,
            send_sem=e["send"].at[self.g, self.p, index],
            recv_sem=e["recv"].at[self.g, self.p, index],
            device_id=(e["s"], e["y"] * SIDE + e["x"]),
            device_id_type=MESH,
        ).wait_recv()
        for eu, ev in self.sends().get((du, dv), []):
            self.copy(du, dv, eu, ev).start()

    def drain(self):
        for (du, dv), targets in self.sends().items():
            for eu, ev in targets:
                self.copy(du, dv, eu, ev).wait_send()


def gather_all(trees):
    for step in range(len(trees[0].order())):
        for tree in trees:
            tree.arrive(*tree.order()[step])


def column(row):
    return jnp.swapaxes(jnp.broadcast_to(row, (LANES, LANES)), 0, 1)


def kernel(
    ns,
    stream, doc, wv, wg, ck, cg, cs, wp, og, osh,
    out,
    gbuf, wvg, wpb, ckv, cgv, csv, ogv, osv, docv, docs, nleft, nright, glu, hsend, hrecv, act, keep, z32, stat,
    stsend, strecv,
    load, send, recv, hss, hrs, dss, drs, ss, sr,
):
    rows = stream.shape[0]
    s = lax.axis_index("sp")
    t = lax.axis_index("tp")
    y, x = t // SIDE, t % SIDE
    env = dict(s=s, x=x, y=y, gbuf=gbuf, send=send, recv=recv)
    after, before = lax.rem(s + 1, ns), lax.rem(s + ns - 1, ns)

    loads = [pltpu.make_async_copy(stream, gbuf.at[0, t], load.at[0])]
    loads.append(pltpu.make_async_copy(doc, docv, load.at[1]))
    for n, (src, dst) in enumerate(((ck, ckv), (cg, cgv), (cs, csv), (og, ogv), (osh, osv))):
        loads.append(pltpu.make_async_copy(src, dst, load.at[2 + n]))
    weights = []
    for layer in range(LAYERS):
        weights.append([
            pltpu.make_async_copy(wv.at[layer], wvg.at[layer, :, pl.ds(0, LANES)], load.at[7 + 3 * layer]),
            pltpu.make_async_copy(wg.at[layer], wvg.at[layer, :, pl.ds(LANES, LANES)], load.at[8 + 3 * layer]),
            pltpu.make_async_copy(wp.at[layer], wpb.at[layer], load.at[9 + 3 * layer]),
        ])
    for c in loads:
        c.start()
    for group in weights:
        for c in group:
            c.start()

    barrier = pltpu.get_barrier_semaphore()
    for d in range(1, PEERS):
        pl.semaphore_signal(barrier, inc=1, device_id=(s, lax.rem(t + d, PEERS)), device_id_type=MESH)
    for other in (after, before):
        pl.semaphore_signal(barrier, inc=1, device_id=(other, t), device_id_type=MESH)
    loads[0].wait()
    pl.semaphore_wait(barrier, PEERS + 1)

    quarter = rows // 4

    def trees_of(g):
        return [Tree(env, g, p, p * quarter, quarter, p % 2 == 0, p < 2) for p in range(4)]

    def halo(src, dst, sem_s, sem_r, who):
        return pltpu.make_async_remote_copy(
            src_ref=src, dst_ref=dst, send_sem=sem_s, recv_sem=sem_r, device_id=(who, t), device_id_type=MESH
        )

    trees = trees_of(0)
    for tree in trees:
        tree.start()

    loads[1].wait()
    for n in range(rows // LANES):
        docs[PAD + n * LANES : PAD + (n + 1) * LANES, :] = column(
            docv[0:1, n * LANES : (n + 1) * LANES].astype(jnp.float32)
        )
    right_doc = halo(docs.at[pl.ds(rows, PAD)], docs.at[pl.ds(0, PAD)], dss.at[0], drs.at[0], after)
    left_doc = halo(docs.at[pl.ds(PAD, PAD)], docs.at[pl.ds(rows + PAD, PAD)], dss.at[1], drs.at[1], before)
    right_doc.start()
    left_doc.start()
    for c in loads[2:]:
        c.wait()
    for group in weights:
        for c in group:
            c.wait()
    right_doc.wait()
    left_doc.wait()

    @pl.when(s == 0)
    def _():
        docs[0:PAD, :] = jnp.full((PAD, LANES), -1.0, jnp.float32)

    @pl.when(s == ns - 1)
    def _():
        docs[rows + PAD : rows + 2 * PAD, :] = jnp.full((PAD, LANES), -1.0, jnp.float32)

    def reach(n, carry):
        base = pl.multiple_of(n * PAD, PAD)
        mine = docs[pl.ds(base + PAD, PAD), :]
        low = jnp.zeros((PAD, LANES), jnp.float32)
        high = jnp.zeros((PAD, LANES), jnp.float32)
        for j in range(1, HALF + 1):
            low = low + (docs[pl.ds(base + PAD - j, PAD), :] == mine).astype(jnp.float32)
            high = high + (docs[pl.ds(base + PAD + j, PAD), :] == mine).astype(jnp.float32)
        nleft[pl.ds(base, PAD), :] = low
        nright[pl.ds(base, PAD), :] = high
        return carry

    lax.fori_loop(0, rows // PAD, reach, 0)

    def conv_tile(layer, base):
        low = nleft[pl.ds(base, PAD), :]
        high = nright[pl.ds(base, PAD), :]
        taps = ckv[layer].astype(jnp.float32)
        total = glu[pl.ds(base + PAD, PAD), :] * taps[HALF : HALF + 1, :]
        for j in range(1, HALF + 1):
            a = glu[pl.ds(base + PAD - j, PAD), :]
            b = glu[pl.ds(base + PAD + j, PAD), :]
            total = total + jnp.where(low >= j, a, 0.0) * taps[HALF - j : HALF - j + 1, :]
            total = total + jnp.where(high >= j, b, 0.0) * taps[HALF + j : HALF + j + 1, :]
        gbuf[2 * layer + 1, t, pl.ds(base, PAD), :] = total.astype(jnp.bfloat16)

    group = 96

    def normed(g, layer, gain, shift, silu):
        def body(n, carry):
            base = pl.multiple_of(n * group, 32)
            one = jnp.zeros((group, LANES), jnp.float32)
            two = jnp.zeros((group, LANES), jnp.float32)
            for j in range(PEERS):
                v = gbuf[g, j, pl.ds(base, group), :].astype(jnp.float32)
                one = one + v
                two = two + v * v
            width = PEERS * LANES
            mean = jnp.sum(one, axis=1, keepdims=True) * (1.0 / width)
            var = jnp.maximum(jnp.sum(two, axis=1, keepdims=True) * (1.0 / width) - mean * mean, 0.0)
            scale = lax.rsqrt(var + EPS)
            for j in range(PEERS):
                v = gbuf[g, j, pl.ds(base, group), :].astype(jnp.float32)
                cols = slice(j * LANES, (j + 1) * LANES)
                v = (v - mean) * scale * gain[layer : layer + 1, cols] + shift[layer : layer + 1, cols]
                if silu:
                    v = v / (1.0 + jnp.exp(-v))
                act[j, pl.ds(base, group), :] = v.astype(jnp.bfloat16)
            return carry

        lax.fori_loop(0, rows // group, body, 0)

    half = rows // 2
    for layer in range(LAYERS):
        g = 2 * layer
        gather_all(trees)
        if layer == 0:
            keep[...] = gbuf[0, t].astype(jnp.float32)
        else:
            normed(g, layer - 1, ogv, osv, False)
            keep[...] = act[t].astype(jnp.float32)
        for h in range(2):
            part = slice(h * half, (h + 1) * half)
            if layer == 0:
                lhs = jnp.concatenate([gbuf[0, j, part, :] for j in range(PEERS)], axis=1)
            else:
                lhs = jnp.concatenate([act[j, part, :] for j in range(PEERS)], axis=1)
            both = jnp.dot(lhs, wvg[layer], preferred_element_type=jnp.float32)
            lin, gat = both[:, :LANES], both[:, LANES:]
            value = (lin / (1.0 + jnp.exp(-gat))).astype(jnp.bfloat16)
            glu[PAD + h * half : PAD + (h + 1) * half, :] = value.astype(jnp.float32)
            if h == 0:
                hsend[layer, 0] = value[:PAD]
            else:
                hsend[layer, 1] = value[half - PAD :]
        right = halo(hsend.at[layer, 1], hrecv.at[layer, 0], hss.at[layer, 0], hrs.at[layer, 0], after)
        left = halo(hsend.at[layer, 0], hrecv.at[layer, 1], hss.at[layer, 1], hrs.at[layer, 1], before)
        right.start()
        left.start()
        for tree in trees:
            tree.drain()

        def inner(n, carry):
            conv_tile(layer, pl.multiple_of(n * PAD, PAD))
            return carry

        lax.fori_loop(1, rows // PAD - 1, inner, 0)
        right.wait()
        left.wait()
        glu[0:PAD, :] = hrecv[layer, 0].astype(jnp.float32)
        glu[rows + PAD : rows + 2 * PAD, :] = hrecv[layer, 1].astype(jnp.float32)
        conv_tile(layer, 0)
        conv_tile(layer, rows - PAD)

        trees = trees_of(g + 1)
        for tree in trees:
            tree.start()
        gather_all(trees)
        normed(g + 1, layer, cgv, csv, True)
        for h in range(2):
            part = slice(h * half, (h + 1) * half)
            lhs = jnp.concatenate([act[j, part, :] for j in range(PEERS)], axis=1)
            z = ALPHA * keep[part, :] + jnp.dot(lhs, wpb[layer], preferred_element_type=jnp.float32)
            if layer < LAYERS - 1:
                gbuf[g + 2, t, part, :] = z.astype(jnp.bfloat16)
            else:
                z32[part, :] = z
        for tree in trees:
            tree.drain()
        if layer < LAYERS - 1:
            trees = trees_of(g + 2)
            for tree in trees:
                tree.start()

    ones = jnp.ones((8, LANES), jnp.float32)
    z = z32[...]
    contract = (((1,), (1,)), ((), ()))
    one = lax.dot_general(ones, z, contract, precision=lax.Precision.HIGHEST, preferred_element_type=jnp.float32)
    two = lax.dot_general(ones, z * z, contract, precision=lax.Precision.HIGHEST, preferred_element_type=jnp.float32)
    stsend[0:1, :] = one[0:1, :]
    stsend[1:2, :] = two[0:1, :]
    outgoing = []
    for d in range(1, PEERS):
        c = pltpu.make_async_remote_copy(
            src_ref=stsend,
            dst_ref=strecv.at[d],
            send_sem=ss.at[d],
            recv_sem=sr.at[d],
            device_id=(s, lax.rem(t + d, PEERS)),
            device_id_type=MESH,
        )
        c.start()
        outgoing.append(c)
    sums = stsend[...]
    for d in range(1, PEERS):
        outgoing[d - 1].wait_recv()
        sums = sums + strecv[d]
    stat[...] = sums
    mine = pl.ds(pl.multiple_of(t * LANES, LANES), LANES)
    gain = ogv[LAYERS - 1 : LAYERS, mine]
    shift = osv[LAYERS - 1 : LAYERS, mine]
    width = PEERS * LANES
    for n in range(rows // LANES):
        cols = slice(n * LANES, (n + 1) * LANES)
        mean = column(stat[0:1, cols]) * (1.0 / width)
        var = jnp.maximum(column(stat[1:2, cols]) * (1.0 / width) - mean * mean, 0.0)
        v = (z32[cols, :] - mean) * lax.rsqrt(var + EPS) * gain + shift
        out[cols, :] = v.astype(jnp.bfloat16)
    for c in outgoing:
        c.wait_send()


def on_device(ns, stream, doc_ids, w_value, w_gate, conv_kernel, conv_gain, conv_shift, w_proj, out_gain, out_shift):
    rows, width = stream.shape[0], w_value.shape[1]
    gathers = 2 * LAYERS
    bf16, f32 = jnp.bfloat16, jnp.float32
    dma = pltpu.SemaphoreType.DMA
    return pl.pallas_call(
        functools.partial(kernel, ns),
        out_shape=jax.ShapeDtypeStruct((rows, LANES), bf16),
        in_specs=[pl.BlockSpec(memory_space=pl.ANY)] * 10,
        out_specs=pl.BlockSpec(memory_space=pltpu.VMEM),
        scratch_shapes=[
            pltpu.VMEM((gathers, PEERS, rows, LANES), bf16),
            pltpu.VMEM((LAYERS, width, 2 * LANES), bf16),
            pltpu.VMEM((LAYERS, width, LANES), bf16),
            pltpu.VMEM((LAYERS, KERNEL, LANES), bf16),
            pltpu.VMEM((LAYERS, width), f32),
            pltpu.VMEM((LAYERS, width), f32),
            pltpu.VMEM((LAYERS, width), f32),
            pltpu.VMEM((LAYERS, width), f32),
            pltpu.VMEM((1, rows), jnp.int32),
            pltpu.VMEM((rows + 2 * PAD, LANES), f32),
            pltpu.VMEM((rows, LANES), f32),
            pltpu.VMEM((rows, LANES), f32),
            pltpu.VMEM((rows + 2 * PAD, LANES), f32),
            pltpu.VMEM((LAYERS, 2, PAD, LANES), bf16),
            pltpu.VMEM((LAYERS, 2, PAD, LANES), bf16),
            pltpu.VMEM((PEERS, rows, LANES), bf16),
            pltpu.VMEM((rows, LANES), f32),
            pltpu.VMEM((rows, LANES), f32),
            pltpu.VMEM((2, rows), f32),
            pltpu.VMEM((2, rows), f32),
            pltpu.VMEM((PEERS, 2, rows), f32),
            dma((7 + 3 * LAYERS,)),
            dma((gathers, 4, PEERS)),
            dma((gathers, 4, PEERS)),
            dma((LAYERS, 2)),
            dma((LAYERS, 2)),
            dma((2,)),
            dma((2,)),
            dma((PEERS,)),
            dma((PEERS,)),
        ],
        compiler_params=pltpu.CompilerParams(
            collective_id=0, has_side_effects=True, vmem_limit_bytes=60 * 1024 * 1024
        ),
        name="stack",
    )(stream, doc_ids.reshape(1, rows), w_value, w_gate, conv_kernel, conv_gain, conv_shift, w_proj, out_gain, out_shift)


def solution(mesh):
    return jax.shard_map(
        functools.partial(on_device, mesh.shape["sp"]),
        mesh=mesh,
        in_specs=(
            P("sp", "tp"), P("sp"), P(None, None, "tp"), P(None, None, "tp"), P(None, None, "tp"), P(), P(),
            P(None, None, "tp"), P(), P(),
        ),
        out_specs=P("sp", "tp"),
        check_vma=False,
    )
```

```python
import functools

import jax
import jax.numpy as jnp
from jax import lax
from jax.experimental import pallas as pl
from jax.experimental.pallas import tpu as pltpu
from jax.sharding import PartitionSpec as P

LAYERS = 3
KERNEL = 31
HALF = 15
PAD = 16
LANES = 128
SIDE = 4
PEERS = SIDE * SIDE
STEPS = (1, -1, 2)
CHUNKS = 3
OUTER = 80
MIDDLE = 144
ALPHA = 2.0**0.25
EPS = 1e-05
MESH = pl.DeviceIdType.MESH


class Spread:
    def __init__(self, env, stage, piece, row0, rows, x_first):
        self.env, self.k, self.p = env, stage, piece
        self.row0, self.rows, self.x_first = row0, rows, x_first

    def at(self, du, dv):
        dx, dy = (du, dv) if self.x_first else (dv, du)
        e = self.env
        return lax.rem(e["y"] + dy + SIDE, SIDE) * SIDE + lax.rem(e["x"] + dx + SIDE, SIDE)

    def ref(self, slot):
        return self.env["gbuf"].at[self.k, slot, pl.ds(self.row0, self.rows), :]

    def copy(self, src, dst, recv, peer):
        e = self.env
        return pltpu.make_async_remote_copy(
            src_ref=src,
            dst_ref=dst,
            send_sem=e["send"].at[self.k, self.p],
            recv_sem=e["recv"].at[self.k, self.p, recv],
            device_id=(e["s"], peer),
            device_id_type=MESH,
        )

    def spread(self, du):
        mine = self.ref(self.at(du, 0))
        for dv in (2, 1, -1):
            self.copy(mine, mine, 3, self.at(0, dv)).start()

    def start(self):
        mine = self.ref(self.at(0, 0))
        for n, du in enumerate(STEPS):
            self.copy(mine, mine, n, self.at(-du, 0)).start()
        self.spread(0)

    def turn(self):
        for n, du in enumerate(STEPS):
            block = self.ref(self.at(du, 0))
            self.copy(block, block, n, self.at(1, 0)).wait_recv()
            self.spread(du)

    def finish(self):
        many = self.ref(pl.ds(0, PEERS - SIDE))
        self.copy(many, many, 3, self.at(1, 0)).wait_recv()

    def drain(self):
        many = self.ref(pl.ds(0, PEERS - 1))
        self.copy(many, many, 3, self.at(1, 0)).wait_send()


def bounds(rows):
    outer, middle = OUTER, MIDDLE
    cuts = []
    for k in range(2 * LAYERS):
        lost = PAD * ((k + 1) // 2)
        cuts.append((0, outer - lost, middle - lost, rows // 2))
    return cuts


def plan(cuts):
    now, link, order = 0.0, 0.0, []
    ready = {("turn", c, 0): 3.0 + 0.5 * c for c in range(CHUNKS)}
    done = set()

    def rows_of(c, k):
        return 2 * (cuts[k][c + 1] - cuts[k][c])

    while ready:
        allowed = [
            step for step in ready
            if step[0] != "conv" or all(("finish", c, step[2]) in done for c in range(step[1]))
        ]
        step = min(allowed, key=lambda each: (max(ready[each], now), ready[each], each[1]))
        what, c, k = step
        now = max(now, ready.pop(step))
        order.append(step)
        done.add(step)
        if what == "turn":
            now += 0.15
            link = max(now + 3.0, link) + 0.02 * rows_of(c, k)
            ready["finish", c, k] = link
        elif what == "finish" and k % 2 == 0:
            now += 0.4 + 0.005 * rows_of(c, k)
            ready["conv", c, k] = now + (2.5 if c == 0 else 0.0)
        elif what == "finish":
            now += 0.4 + 0.008 * rows_of(c, k)
            if k + 1 < 2 * LAYERS:
                ready["turn", c, k + 1] = now + 3.0
        else:
            now += 0.2 + 0.003 * rows_of(c, k)
            ready["turn", c, k + 1] = now + 3.0
    return order


def column(row):
    return jnp.swapaxes(jnp.broadcast_to(row, (LANES, LANES)), 0, 1)


def kernel(
    ns,
    stream, doc, wv, wg, ck, cg, cs, wp, og, osh,
    out,
    gbuf, wvg, wpb, ckv, cgv, csv, ogv, osv, docv, docs, nleft, nright, glu, hsend, hrecv, act, keep, z32, stat,
    stsend, strecv,
    load, send, recv, hss, hrs, dss, drs, ss, sr,
):
    rows = stream.shape[0]
    s = lax.axis_index("sp")
    t = lax.axis_index("tp")
    y, x = t // SIDE, t % SIDE
    env = dict(s=s, x=x, y=y, gbuf=gbuf, send=send, recv=recv)
    after, before = lax.rem(s + 1, ns), lax.rem(s + ns - 1, ns)

    loads = [pltpu.make_async_copy(stream, gbuf.at[0, t], load.at[0])]
    loads.append(pltpu.make_async_copy(doc, docv, load.at[1]))
    for n, (src, dst) in enumerate(((ck, ckv), (cg, cgv), (cs, csv), (og, ogv), (osh, osv))):
        loads.append(pltpu.make_async_copy(src, dst, load.at[2 + n]))
    weights = []
    for layer in range(LAYERS):
        weights.append([
            pltpu.make_async_copy(wv.at[layer], wvg.at[layer, :, pl.ds(0, LANES)], load.at[7 + 3 * layer]),
            pltpu.make_async_copy(wg.at[layer], wvg.at[layer, :, pl.ds(LANES, LANES)], load.at[8 + 3 * layer]),
            pltpu.make_async_copy(wp.at[layer], wpb.at[layer], load.at[9 + 3 * layer]),
        ])
    for c in loads:
        c.start()
    for group in weights:
        for c in group:
            c.start()

    barrier = pltpu.get_barrier_semaphore()
    for d in range(1, PEERS):
        pl.semaphore_signal(barrier, inc=1, device_id=(s, lax.rem(t + d, PEERS)), device_id_type=MESH)
    for other in (after, before):
        pl.semaphore_signal(barrier, inc=1, device_id=(other, t), device_id_type=MESH)
    loads[0].wait()
    pl.semaphore_wait(barrier, PEERS + 1)

    cuts = bounds(rows)
    pieces = {}
    for k in range(2 * LAYERS):
        for c in range(CHUNKS):
            low, high = cuts[k][c], cuts[k][c + 1]
            pieces[c, k] = (
                Spread(env, k, 2 * c, low, high - low, True),
                Spread(env, k, 2 * c + 1, rows - high, high - low, False),
            )

    def start(c, k):
        for piece in pieces[c, k]:
            piece.start()

    def halo(src, dst, sem_s, sem_r, who):
        return pltpu.make_async_remote_copy(
            src_ref=src, dst_ref=dst, send_sem=sem_s, recv_sem=sem_r, device_id=(who, t), device_id_type=MESH
        )

    for c in range(CHUNKS):
        start(c, 0)

    loads[1].wait()
    for n in range(rows // LANES):
        docs[PAD + n * LANES : PAD + (n + 1) * LANES, :] = column(
            docv[0:1, n * LANES : (n + 1) * LANES].astype(jnp.float32)
        )
    right_doc = halo(docs.at[pl.ds(rows, PAD)], docs.at[pl.ds(0, PAD)], dss.at[0], drs.at[0], after)
    left_doc = halo(docs.at[pl.ds(PAD, PAD)], docs.at[pl.ds(rows + PAD, PAD)], dss.at[1], drs.at[1], before)
    right_doc.start()
    left_doc.start()
    for c in loads[2:]:
        c.wait()
    for group in weights:
        for c in group:
            c.wait()
    right_doc.wait()
    left_doc.wait()

    @pl.when(s == 0)
    def _():
        docs[0:PAD, :] = jnp.full((PAD, LANES), -1.0, jnp.float32)

    @pl.when(s == ns - 1)
    def _():
        docs[rows + PAD : rows + 2 * PAD, :] = jnp.full((PAD, LANES), -1.0, jnp.float32)

    def reach(n, carry):
        base = pl.multiple_of(n * PAD, PAD)
        mine = docs[pl.ds(base + PAD, PAD), :]
        low = jnp.zeros((PAD, LANES), jnp.float32)
        high = jnp.zeros((PAD, LANES), jnp.float32)
        for j in range(1, HALF + 1):
            low = low + (docs[pl.ds(base + PAD - j, PAD), :] == mine).astype(jnp.float32)
            high = high + (docs[pl.ds(base + PAD + j, PAD), :] == mine).astype(jnp.float32)
        nleft[pl.ds(base, PAD), :] = low
        nright[pl.ds(base, PAD), :] = high
        return carry

    lax.fori_loop(0, rows // PAD, reach, 0)

    def conv_rows(layer, first, last):
        def tile(n, carry):
            base = pl.multiple_of(n * PAD, PAD)
            low = nleft[pl.ds(base, PAD), :]
            high = nright[pl.ds(base, PAD), :]
            taps = ckv[layer].astype(jnp.float32)
            total = glu[layer, pl.ds(base + PAD, PAD), :] * taps[HALF : HALF + 1, :]
            for j in range(1, HALF + 1):
                a = glu[layer, pl.ds(base + PAD - j, PAD), :]
                b = glu[layer, pl.ds(base + PAD + j, PAD), :]
                total = total + jnp.where(low >= j, a, 0.0) * taps[HALF - j : HALF - j + 1, :]
                total = total + jnp.where(high >= j, b, 0.0) * taps[HALF + j : HALF + j + 1, :]
            gbuf[2 * layer + 1, t, pl.ds(base, PAD), :] = total.astype(jnp.bfloat16)
            return carry

        lax.fori_loop(first // PAD, last // PAD, tile, 0)

    def normed(k, layer, gain, shift, silu, part):
        count = part.stop - part.start
        one = jnp.zeros((count, LANES), jnp.float32)
        two = jnp.zeros((count, LANES), jnp.float32)
        for j in range(PEERS):
            v = gbuf[k, j, part, :].astype(jnp.float32)
            one = one + v
            two = two + v * v
        width = PEERS * LANES
        mean = jnp.sum(one, axis=1, keepdims=True) * (1.0 / width)
        var = jnp.maximum(jnp.sum(two, axis=1, keepdims=True) * (1.0 / width) - mean * mean, 0.0)
        scale = lax.rsqrt(var + EPS)
        for j in range(PEERS):
            v = gbuf[k, j, part, :].astype(jnp.float32)
            cols = slice(j * LANES, (j + 1) * LANES)
            v = (v - mean) * scale * gain[layer : layer + 1, cols] + shift[layer : layer + 1, cols]
            if silu:
                v = v / (1.0 + jnp.exp(-v))
            act[j, part, :] = v.astype(jnp.bfloat16)

    def halos(layer):
        return [
            halo(hsend.at[layer, 1], hrecv.at[layer, 0], hss.at[layer, 0], hrs.at[layer, 0], after),
            halo(hsend.at[layer, 0], hrecv.at[layer, 1], hss.at[layer, 1], hrs.at[layer, 1], before),
        ]

    def sides(c, k):
        return [slice(p.row0, p.row0 + p.rows) for p in pieces[c, k]]

    def joined(ref, parts):
        rows_of = [jnp.concatenate([ref[j, part, :] for j in range(PEERS)], axis=1) for part in parts]
        return jnp.concatenate(rows_of, axis=0)

    def gated(c, k):
        layer, parts = k // 2, sides(c, k)
        if layer == 0:
            lhs = joined(gbuf.at[0], parts)
            for part in parts:
                keep[part, :] = gbuf[0, t, part, :].astype(jnp.float32)
        else:
            for part in parts:
                normed(k, layer - 1, ogv, osv, False, part)
                keep[part, :] = act[t, part, :].astype(jnp.float32)
            lhs = joined(act, parts)
        both = jnp.dot(lhs, wvg[layer], preferred_element_type=jnp.float32)
        value = (both[:, :LANES] / (1.0 + jnp.exp(-both[:, LANES:]))).astype(jnp.bfloat16)
        count = pieces[c, k][0].rows
        for n, part in enumerate(parts):
            mine = value[n * count : (n + 1) * count]
            glu[layer, PAD + part.start : PAD + part.stop, :] = mine.astype(jnp.float32)
            if c == 0:
                hsend[layer, n] = mine[:PAD] if n == 0 else mine[count - PAD :]
        if c == 0:
            for h in halos(layer):
                h.start()

    def convolved(c, k):
        layer = k // 2
        left, right = sides(c, k + 1)
        if c == 0:
            conv_rows(layer, left.start + PAD, left.stop)
            conv_rows(layer, right.start, right.stop - PAD)
            for h in halos(layer):
                h.wait()
            glu[layer, 0:PAD, :] = hrecv[layer, 0].astype(jnp.float32)
            glu[layer, rows + PAD : rows + 2 * PAD, :] = hrecv[layer, 1].astype(jnp.float32)
            conv_rows(layer, 0, PAD)
            conv_rows(layer, rows - PAD, rows)
        elif left.stop == right.start:
            conv_rows(layer, left.start, right.stop)
        else:
            conv_rows(layer, left.start, left.stop)
            conv_rows(layer, right.start, right.stop)

    def projected(c, k):
        layer, parts = k // 2, sides(c, k)
        for part in parts:
            normed(k, layer, cgv, csv, True, part)
        branch = jnp.dot(joined(act, parts), wpb[layer], preferred_element_type=jnp.float32)
        count = pieces[c, k][0].rows
        for n, part in enumerate(parts):
            z = ALPHA * keep[part, :] + branch[n * count : (n + 1) * count]
            if layer < LAYERS - 1:
                gbuf[k + 1, t, part, :] = z.astype(jnp.bfloat16)
            else:
                z32[part, :] = z

    for what, c, k in plan(cuts):
        if what == "turn":
            for piece in pieces[c, k]:
                piece.turn()
        elif what == "finish":
            for piece in pieces[c, k]:
                piece.finish()
            if k % 2 == 0:
                gated(c, k)
            else:
                projected(c, k)
                if k + 1 < 2 * LAYERS:
                    start(c, k + 1)
        else:
            convolved(c, k)
            start(c, k + 1)

    ones = jnp.ones((8, LANES), jnp.float32)
    z = z32[...]
    contract = (((1,), (1,)), ((), ()))
    one = lax.dot_general(ones, z, contract, precision=lax.Precision.HIGHEST, preferred_element_type=jnp.float32)
    two = lax.dot_general(ones, z * z, contract, precision=lax.Precision.HIGHEST, preferred_element_type=jnp.float32)
    stsend[0:1, :] = one[0:1, :]
    stsend[1:2, :] = two[0:1, :]
    outgoing = []
    for d in range(1, PEERS):
        c = pltpu.make_async_remote_copy(
            src_ref=stsend,
            dst_ref=strecv.at[d],
            send_sem=ss.at[d],
            recv_sem=sr.at[d],
            device_id=(s, lax.rem(t + d, PEERS)),
            device_id_type=MESH,
        )
        c.start()
        outgoing.append(c)
    sums = stsend[...]
    for d in range(1, PEERS):
        outgoing[d - 1].wait_recv()
        sums = sums + strecv[d]
    stat[...] = sums
    mine = pl.ds(pl.multiple_of(t * LANES, LANES), LANES)
    gain = ogv[LAYERS - 1 : LAYERS, mine]
    shift = osv[LAYERS - 1 : LAYERS, mine]
    width = PEERS * LANES
    for n in range(rows // LANES):
        cols = slice(n * LANES, (n + 1) * LANES)
        mean = column(stat[0:1, cols]) * (1.0 / width)
        var = jnp.maximum(column(stat[1:2, cols]) * (1.0 / width) - mean * mean, 0.0)
        v = (z32[cols, :] - mean) * lax.rsqrt(var + EPS) * gain + shift
        out[cols, :] = v.astype(jnp.bfloat16)
    for c in outgoing:
        c.wait_send()
    for pair in pieces.values():
        for piece in pair:
            piece.drain()


def on_device(ns, stream, doc_ids, w_value, w_gate, conv_kernel, conv_gain, conv_shift, w_proj, out_gain, out_shift):
    rows, width = stream.shape[0], w_value.shape[1]
    gathers = 2 * LAYERS
    bf16, f32 = jnp.bfloat16, jnp.float32
    dma = pltpu.SemaphoreType.DMA
    return pl.pallas_call(
        functools.partial(kernel, ns),
        out_shape=jax.ShapeDtypeStruct((rows, LANES), bf16),
        in_specs=[pl.BlockSpec(memory_space=pl.ANY)] * 10,
        out_specs=pl.BlockSpec(memory_space=pltpu.VMEM),
        scratch_shapes=[
            pltpu.VMEM((gathers, PEERS, rows, LANES), bf16),
            pltpu.VMEM((LAYERS, width, 2 * LANES), bf16),
            pltpu.VMEM((LAYERS, width, LANES), bf16),
            pltpu.VMEM((LAYERS, KERNEL, LANES), bf16),
            pltpu.VMEM((LAYERS, width), f32),
            pltpu.VMEM((LAYERS, width), f32),
            pltpu.VMEM((LAYERS, width), f32),
            pltpu.VMEM((LAYERS, width), f32),
            pltpu.VMEM((1, rows), jnp.int32),
            pltpu.VMEM((rows + 2 * PAD, LANES), f32),
            pltpu.VMEM((rows, LANES), f32),
            pltpu.VMEM((rows, LANES), f32),
            pltpu.VMEM((LAYERS, rows + 2 * PAD, LANES), f32),
            pltpu.VMEM((LAYERS, 2, PAD, LANES), bf16),
            pltpu.VMEM((LAYERS, 2, PAD, LANES), bf16),
            pltpu.VMEM((PEERS, rows, LANES), bf16),
            pltpu.VMEM((rows, LANES), f32),
            pltpu.VMEM((rows, LANES), f32),
            pltpu.VMEM((2, rows), f32),
            pltpu.VMEM((2, rows), f32),
            pltpu.VMEM((PEERS, 2, rows), f32),
            dma((7 + 3 * LAYERS,)),
            dma((gathers, 2 * CHUNKS)),
            dma((gathers, 2 * CHUNKS, SIDE)),
            dma((LAYERS, 2)),
            dma((LAYERS, 2)),
            dma((2,)),
            dma((2,)),
            dma((PEERS,)),
            dma((PEERS,)),
        ],
        compiler_params=pltpu.CompilerParams(
            collective_id=0, has_side_effects=True, vmem_limit_bytes=60 * 1024 * 1024
        ),
        name="stack",
    )(stream, doc_ids.reshape(1, rows), w_value, w_gate, conv_kernel, conv_gain, conv_shift, w_proj, out_gain, out_shift)


def solution(mesh):
    return jax.shard_map(
        functools.partial(on_device, mesh.shape["sp"]),
        mesh=mesh,
        in_specs=(
            P("sp", "tp"), P("sp"), P(None, None, "tp"), P(None, None, "tp"), P(None, None, "tp"), P(), P(),
            P(None, None, "tp"), P(), P(),
        ),
        out_specs=P("sp", "tp"),
        check_vma=False,
    )
```

```python
import functools

import jax
import jax.numpy as jnp
from jax import lax
from jax.experimental import pallas as pl
from jax.experimental.pallas import tpu as pltpu
from jax.sharding import PartitionSpec as P

LAYERS = 3
KERNEL = 31
HALF = 15
PAD = 16
LANES = 128
SIDE = 4
PEERS = SIDE * SIDE
STEPS = (1, -1, 2)
SENDS = (2, 1, -1)
FAR_FIRST = [(du, dv) for du in (2, 1, -1, 0) for dv in (2, 1, -1, 0) if (du, dv) != (0, 0)]
CHUNKS = 4
OUTER = 80
MIDDLE = 144
STAGGER = False
DIRECT = (True, False, False, False)
ALPHA = 2.0**0.25
EPS = 1e-05
MESH = pl.DeviceIdType.MESH


class Spread:
    def __init__(self, env, stage, piece, row0, rows, x_first, direct):
        self.env, self.k, self.p, self.direct = env, stage, piece, direct
        self.row0, self.rows, self.x_first = row0, rows, x_first

    def at(self, du, dv):
        dx, dy = (du, dv) if self.x_first else (dv, du)
        e = self.env
        return lax.rem(e["y"] + dy + SIDE, SIDE) * SIDE + lax.rem(e["x"] + dx + SIDE, SIDE)

    def ref(self, slot):
        return self.env["gbuf"].at[self.k, slot, pl.ds(self.row0, self.rows), :]

    def copy(self, src, dst, recv, peer):
        e = self.env
        return pltpu.make_async_remote_copy(
            src_ref=src,
            dst_ref=dst,
            send_sem=e["send"].at[self.k, self.p],
            recv_sem=e["recv"].at[self.k, self.p, recv],
            device_id=(e["s"], peer),
            device_id_type=MESH,
        )

    def spread(self, du):
        mine = self.ref(self.at(du, 0))
        for dv in SENDS:
            self.copy(mine, mine, 3, self.at(0, dv)).start()

    def start(self):
        mine = self.ref(self.at(0, 0))
        if self.direct:
            for du, dv in FAR_FIRST:
                self.copy(mine, mine, 3, self.at(du, dv)).start()
            return
        for du in SENDS:
            self.copy(mine, mine, STEPS.index(du), self.at(-du, 0)).start()
        self.spread(0)

    def turn(self, du):
        block = self.ref(self.at(du, 0))
        self.copy(block, block, STEPS.index(du), self.at(1, 0)).wait_recv()
        self.spread(du)

    def finish(self):
        many = self.ref(pl.ds(0, PEERS - 1 if self.direct else PEERS - SIDE))
        self.copy(many, many, 3, self.at(1, 0)).wait_recv()

    def drain(self):
        many = self.ref(pl.ds(0, PEERS - 1))
        self.copy(many, many, 3, self.at(1, 0)).wait_send()


def bounds(rows):
    outer, middle = OUTER, MIDDLE
    cuts = []
    for k in range(2 * LAYERS):
        lost = PAD * ((k + 1) // 2)
        cuts.append((0, PAD, outer - lost, middle - lost, rows // 2))
    return cuts


def plan():
    order = [("turn", 1, 0), ("turn", 2, 0), ("finish", 0, 0), ("turn", 3, 0)]
    last = 2 * LAYERS - 1
    for k in range(last + 1):
        conv = k % 2 == 0
        order.append(("finish", 1, k))
        if conv:
            order += [("conv", 1, k), ("conv", 0, k)]
        order.append(("finish", 2, k))
        if conv:
            order.append(("conv", 2, k))
        if STAGGER and k < last:
            order += [("turn", 1, k + 1), ("finish", 0, k + 1)]
        order.append(("finish", 3, k))
        if conv:
            order.append(("conv", 3, k))
        if k < last:
            if not STAGGER:
                order += [("turn", 1, k + 1), ("finish", 0, k + 1)]
            order += [("turn", 2, k + 1), ("turn", 3, k + 1)]
    return order


def column(row):
    return jnp.swapaxes(jnp.broadcast_to(row, (LANES, LANES)), 0, 1)


def kernel(
    ns,
    stream, doc, wv, wg, ck, cg, cs, wp, og, osh,
    out,
    gbuf, wvg, wpb, ckv, cgv, csv, ogv, osv, docv, docs, nleft, nright, glu, hsend, hrecv, act, keep, z32, stat,
    stsend, strecv,
    load, send, recv, hss, hrs, dss, drs, ss, sr,
):
    rows = stream.shape[0]
    s = lax.axis_index("sp")
    t = lax.axis_index("tp")
    y, x = t // SIDE, t % SIDE
    env = dict(s=s, x=x, y=y, gbuf=gbuf, send=send, recv=recv)
    after, before = lax.rem(s + 1, ns), lax.rem(s + ns - 1, ns)

    loads = [pltpu.make_async_copy(stream, gbuf.at[0, t], load.at[0])]
    loads.append(pltpu.make_async_copy(doc, docv, load.at[1]))
    for n, (src, dst) in enumerate(((ck, ckv), (cg, cgv), (cs, csv), (og, ogv), (osh, osv))):
        loads.append(pltpu.make_async_copy(src, dst, load.at[2 + n]))
    weights = []
    for layer in range(LAYERS):
        weights.append([
            pltpu.make_async_copy(wv.at[layer], wvg.at[layer, :, pl.ds(0, LANES)], load.at[7 + 3 * layer]),
            pltpu.make_async_copy(wg.at[layer], wvg.at[layer, :, pl.ds(LANES, LANES)], load.at[8 + 3 * layer]),
            pltpu.make_async_copy(wp.at[layer], wpb.at[layer], load.at[9 + 3 * layer]),
        ])
    for c in loads:
        c.start()
    for group in weights:
        for c in group:
            c.start()

    barrier = pltpu.get_barrier_semaphore()
    for d in range(1, PEERS):
        pl.semaphore_signal(barrier, inc=1, device_id=(s, lax.rem(t + d, PEERS)), device_id_type=MESH)
    for other in (after, before):
        pl.semaphore_signal(barrier, inc=1, device_id=(other, t), device_id_type=MESH)
    loads[0].wait()
    pl.semaphore_wait(barrier, PEERS + 1)

    cuts = bounds(rows)
    pieces = {}
    for k in range(2 * LAYERS):
        for c in range(CHUNKS):
            low, high = cuts[k][c], cuts[k][c + 1]
            pieces[c, k] = (
                Spread(env, k, 2 * c, low, high - low, True, DIRECT[c]),
                Spread(env, k, 2 * c + 1, rows - high, high - low, False, DIRECT[c]),
            )

    def start(c, k):
        for piece in pieces[c, k]:
            piece.start()

    def halo(src, dst, sem_s, sem_r, who):
        return pltpu.make_async_remote_copy(
            src_ref=src, dst_ref=dst, send_sem=sem_s, recv_sem=sem_r, device_id=(who, t), device_id_type=MESH
        )

    for c in range(CHUNKS):
        start(c, 0)

    loads[1].wait()
    for n in range(rows // LANES):
        docs[PAD + n * LANES : PAD + (n + 1) * LANES, :] = column(
            docv[n * LANES : (n + 1) * LANES].astype(jnp.float32).reshape(1, LANES)
        )
    right_doc = halo(docs.at[pl.ds(rows, PAD)], docs.at[pl.ds(0, PAD)], dss.at[0], drs.at[0], after)
    left_doc = halo(docs.at[pl.ds(PAD, PAD)], docs.at[pl.ds(rows + PAD, PAD)], dss.at[1], drs.at[1], before)
    right_doc.start()
    left_doc.start()
    def prepare():
        for c in loads[2:]:
            c.wait()
        right_doc.wait()
        left_doc.wait()

        @pl.when(s == 0)
        def _():
            docs[0:PAD, :] = jnp.full((PAD, LANES), -1.0, jnp.float32)

        @pl.when(s == ns - 1)
        def _():
            docs[rows + PAD : rows + 2 * PAD, :] = jnp.full((PAD, LANES), -1.0, jnp.float32)

        def reach(n, carry):
            base = pl.multiple_of(n * PAD, PAD)
            mine = docs[pl.ds(base + PAD, PAD), :]
            low = jnp.zeros((PAD, LANES), jnp.float32)
            high = jnp.zeros((PAD, LANES), jnp.float32)
            for j in range(1, HALF + 1):
                low = low + (docs[pl.ds(base + PAD - j, PAD), :] == mine).astype(jnp.float32)
                high = high + (docs[pl.ds(base + PAD + j, PAD), :] == mine).astype(jnp.float32)
            nleft[pl.ds(base, PAD), :] = low
            nright[pl.ds(base, PAD), :] = high
            return carry

        lax.fori_loop(0, rows // PAD, reach, 0)

    def conv_rows(layer, first, last):
        def tile(n, carry):
            base = pl.multiple_of(n * PAD, PAD)
            low = nleft[pl.ds(base, PAD), :]
            high = nright[pl.ds(base, PAD), :]
            taps = ckv[layer].astype(jnp.float32)
            total = glu[layer, pl.ds(base + PAD, PAD), :] * taps[HALF : HALF + 1, :]
            for j in range(1, HALF + 1):
                a = glu[layer, pl.ds(base + PAD - j, PAD), :]
                b = glu[layer, pl.ds(base + PAD + j, PAD), :]
                total = total + jnp.where(low >= j, a, 0.0) * taps[HALF - j : HALF - j + 1, :]
                total = total + jnp.where(high >= j, b, 0.0) * taps[HALF + j : HALF + j + 1, :]
            gbuf[2 * layer + 1, t, pl.ds(base, PAD), :] = total.astype(jnp.bfloat16)
            return carry

        lax.fori_loop(first // PAD, last // PAD, tile, 0)

    def normed(k, layer, gain, shift, silu, part):
        count = part.stop - part.start
        one = jnp.zeros((count, LANES), jnp.float32)
        two = jnp.zeros((count, LANES), jnp.float32)
        for j in range(PEERS):
            v = gbuf[k, j, part, :].astype(jnp.float32)
            one = one + v
            two = two + v * v
        width = PEERS * LANES
        mean = jnp.sum(one, axis=1, keepdims=True) * (1.0 / width)
        var = jnp.maximum(jnp.sum(two, axis=1, keepdims=True) * (1.0 / width) - mean * mean, 0.0)
        scale = lax.rsqrt(var + EPS)
        centre = mean * scale
        for j in range(PEERS):
            v = gbuf[k, j, part, :].astype(jnp.float32)
            cols = slice(j * LANES, (j + 1) * LANES)
            factor, offset = gain[layer : layer + 1, cols], shift[layer : layer + 1, cols]
            if silu:
                factor, offset = 0.5 * factor, 0.5 * offset
            v = (v * scale - centre) * factor + offset
            if silu:
                v = v + v * jnp.tanh(v)
            act[j, part, :] = v.astype(jnp.bfloat16)

    def halos(layer):
        return [
            halo(hsend.at[layer, 1], hrecv.at[layer, 0], hss.at[layer, 0], hrs.at[layer, 0], after),
            halo(hsend.at[layer, 0], hrecv.at[layer, 1], hss.at[layer, 1], hrs.at[layer, 1], before),
        ]

    def sides(c, k):
        return [slice(p.row0, p.row0 + p.rows) for p in pieces[c, k]]

    def joined(ref, parts):
        rows_of = [jnp.concatenate([ref[j, part, :] for j in range(PEERS)], axis=1) for part in parts]
        return jnp.concatenate(rows_of, axis=0)

    pending = {(layer, n) for layer in range(LAYERS) for n in range(2)}

    def loaded(layer, n):
        if (layer, n) in pending:
            pending.remove((layer, n))
            for c in weights[layer][2:] if n else weights[layer][:2]:
                c.wait()

    def gated(c, k):
        layer, parts = k // 2, sides(c, k)
        loaded(layer, 0)
        if layer == 0:
            lhs = joined(gbuf.at[0], parts)
            for part in parts:
                keep[part, :] = gbuf[0, t, part, :].astype(jnp.float32)
        else:
            for part in parts:
                normed(k, layer - 1, ogv, osv, False, part)
                keep[part, :] = act[t, part, :].astype(jnp.float32)
            lhs = joined(act, parts)
        both = jnp.dot(lhs, wvg[layer], preferred_element_type=jnp.float32)
        value = (both[:, :LANES] / (1.0 + jnp.exp(-both[:, LANES:]))).astype(jnp.bfloat16)
        count = pieces[c, k][0].rows
        for n, part in enumerate(parts):
            mine = value[n * count : (n + 1) * count]
            glu[layer, PAD + part.start : PAD + part.stop, :] = mine.astype(jnp.float32)
            if c == 0:
                hsend[layer, n] = mine[:PAD] if n == 0 else mine[count - PAD :]
        if c == 0:
            for h in halos(layer):
                h.start()

    def convolved(c, k):
        layer = k // 2
        left, right = sides(c, k + 1)
        if c == 0:
            for h in halos(layer):
                h.wait()
            glu[layer, 0:PAD, :] = hrecv[layer, 0].astype(jnp.float32)
            glu[layer, rows + PAD : rows + 2 * PAD, :] = hrecv[layer, 1].astype(jnp.float32)
            conv_rows(layer, 0, PAD)
            conv_rows(layer, rows - PAD, rows)
        elif left.stop == right.start:
            conv_rows(layer, left.start, right.stop)
        else:
            conv_rows(layer, left.start, left.stop)
            conv_rows(layer, right.start, right.stop)

    def projected(c, k):
        layer, parts = k // 2, sides(c, k)
        loaded(layer, 1)
        for part in parts:
            normed(k, layer, cgv, csv, True, part)
        branch = jnp.dot(joined(act, parts), wpb[layer], preferred_element_type=jnp.float32)
        count = pieces[c, k][0].rows
        for n, part in enumerate(parts):
            z = ALPHA * keep[part, :] + branch[n * count : (n + 1) * count]
            if layer < LAYERS - 1:
                gbuf[k + 1, t, part, :] = z.astype(jnp.bfloat16)
            else:
                z32[part, :] = z

    order = plan()
    waiting = CHUNKS - sum(DIRECT)
    for what, c, k in order:
        if waiting and what == "turn":
            waiting -= 1
        elif waiting == 0 or (waiting and what == "conv"):
            prepare()
            waiting = None
        if what == "turn":
            for du in STEPS:
                for piece in pieces[c, k]:
                    piece.turn(du)
        elif what == "finish":
            for piece in pieces[c, k]:
                piece.finish()
            if k % 2 == 0:
                gated(c, k)
            else:
                projected(c, k)
                if k + 1 < 2 * LAYERS:
                    start(c, k + 1)
        else:
            convolved(c, k)
            start(c, k + 1)

    ones = jnp.ones((8, LANES), jnp.float32)
    z = z32[...]
    contract = (((1,), (1,)), ((), ()))
    one = lax.dot_general(ones, z, contract, precision=lax.Precision.HIGHEST, preferred_element_type=jnp.float32)
    two = lax.dot_general(ones, z * z, contract, precision=lax.Precision.HIGHEST, preferred_element_type=jnp.float32)
    stsend[0:1, :] = one[0:1, :]
    stsend[1:2, :] = two[0:1, :]
    outgoing = []
    for d in range(1, PEERS):
        c = pltpu.make_async_remote_copy(
            src_ref=stsend,
            dst_ref=strecv.at[d],
            send_sem=ss.at[d],
            recv_sem=sr.at[d],
            device_id=(s, lax.rem(t + d, PEERS)),
            device_id_type=MESH,
        )
        c.start()
        outgoing.append(c)
    sums = stsend[...]
    for d in range(1, PEERS):
        outgoing[d - 1].wait_recv()
        sums = sums + strecv[d]
    stat[...] = sums
    mine = pl.ds(pl.multiple_of(t * LANES, LANES), LANES)
    gain = ogv[LAYERS - 1 : LAYERS, mine]
    shift = osv[LAYERS - 1 : LAYERS, mine]
    width = PEERS * LANES
    for n in range(rows // LANES):
        cols = slice(n * LANES, (n + 1) * LANES)
        mean = column(stat[0:1, cols]) * (1.0 / width)
        var = jnp.maximum(column(stat[1:2, cols]) * (1.0 / width) - mean * mean, 0.0)
        v = (z32[cols, :] - mean) * lax.rsqrt(var + EPS) * gain + shift
        out[cols, :] = v.astype(jnp.bfloat16)
    for c in outgoing:
        c.wait_send()
    for pair in pieces.values():
        for piece in pair:
            piece.drain()


def on_device(ns, stream, doc_ids, w_value, w_gate, conv_kernel, conv_gain, conv_shift, w_proj, out_gain, out_shift):
    rows, width = stream.shape[0], w_value.shape[1]
    gathers = 2 * LAYERS
    bf16, f32 = jnp.bfloat16, jnp.float32
    dma = pltpu.SemaphoreType.DMA
    return pl.pallas_call(
        functools.partial(kernel, ns),
        out_shape=jax.ShapeDtypeStruct((rows, LANES), bf16),
        in_specs=[pl.BlockSpec(memory_space=pl.ANY)] * 10,
        out_specs=pl.BlockSpec(memory_space=pltpu.VMEM),
        scratch_shapes=[
            pltpu.VMEM((gathers, PEERS, rows, LANES), bf16),
            pltpu.VMEM((LAYERS, width, 2 * LANES), bf16),
            pltpu.VMEM((LAYERS, width, LANES), bf16),
            pltpu.VMEM((LAYERS, KERNEL, LANES), bf16),
            pltpu.VMEM((LAYERS, width), f32),
            pltpu.VMEM((LAYERS, width), f32),
            pltpu.VMEM((LAYERS, width), f32),
            pltpu.VMEM((LAYERS, width), f32),
            pltpu.VMEM((rows,), jnp.int32),
            pltpu.VMEM((rows + 2 * PAD, LANES), f32),
            pltpu.VMEM((rows, LANES), f32),
            pltpu.VMEM((rows, LANES), f32),
            pltpu.VMEM((LAYERS, rows + 2 * PAD, LANES), f32),
            pltpu.VMEM((LAYERS, 2, PAD, LANES), bf16),
            pltpu.VMEM((LAYERS, 2, PAD, LANES), bf16),
            pltpu.VMEM((PEERS, rows, LANES), bf16),
            pltpu.VMEM((rows, LANES), f32),
            pltpu.VMEM((rows, LANES), f32),
            pltpu.VMEM((2, rows), f32),
            pltpu.VMEM((2, rows), f32),
            pltpu.VMEM((PEERS, 2, rows), f32),
            dma((7 + 3 * LAYERS,)),
            dma((gathers, 2 * CHUNKS)),
            dma((gathers, 2 * CHUNKS, SIDE)),
            dma((LAYERS, 2)),
            dma((LAYERS, 2)),
            dma((2,)),
            dma((2,)),
            dma((PEERS,)),
            dma((PEERS,)),
        ],
        compiler_params=pltpu.CompilerParams(
            collective_id=0, has_side_effects=True, vmem_limit_bytes=60 * 1024 * 1024
        ),
        name="stack",
    )(stream, doc_ids, w_value, w_gate, conv_kernel, conv_gain, conv_shift, w_proj, out_gain, out_shift)


def solution(mesh):
    return jax.shard_map(
        functools.partial(on_device, mesh.shape["sp"]),
        mesh=mesh,
        in_specs=(
            P("sp", "tp"), P("sp"), P(None, None, "tp"), P(None, None, "tp"), P(None, None, "tp"), P(), P(),
            P(None, None, "tp"), P(), P(),
        ),
        out_specs=P("sp", "tp"),
        check_vma=False,
    )
```

```python
import functools

import jax
import jax.numpy as jnp
from jax import lax
from jax.experimental import pallas as pl
from jax.experimental.pallas import tpu as pltpu
from jax.sharding import PartitionSpec as P

LAYERS = 3
KERNEL = 31
HALF = 15
PAD = 16
LANES = 128
SIDE = 4
PEERS = SIDE * SIDE
STEPS = (1, -1, 2)
SENDS = (2, 1, -1)
FAR_FIRST = [(du, dv) for du in (2, 1, -1, 0) for dv in (2, 1, -1, 0) if (du, dv) != (0, 0)]
CHUNKS = 4
OUTER = 96
MIDDLE = 160
EDGE_AFTER = 1
DIRECT = (True, False, False, False)
ALPHA = 2.0**0.25
EPS = 1e-05
MESH = pl.DeviceIdType.MESH


class Spread:
    def __init__(self, env, stage, piece, row0, rows, x_first, direct):
        self.env, self.k, self.p, self.direct = env, stage, piece, direct
        self.row0, self.rows, self.x_first = row0, rows, x_first

    def at(self, du, dv):
        dx, dy = (du, dv) if self.x_first else (dv, du)
        e = self.env
        return lax.rem(e["y"] + dy + SIDE, SIDE) * SIDE + lax.rem(e["x"] + dx + SIDE, SIDE)

    def ref(self, slot):
        return self.env["gbuf"].at[self.k, slot, pl.ds(self.row0, self.rows), :]

    def copy(self, src, dst, recv, peer):
        e = self.env
        return pltpu.make_async_remote_copy(
            src_ref=src,
            dst_ref=dst,
            send_sem=e["send"].at[self.k, self.p],
            recv_sem=e["recv"].at[self.k, self.p, recv],
            device_id=(e["s"], peer),
            device_id_type=MESH,
        )

    def spread(self, du):
        mine = self.ref(self.at(du, 0))
        for dv in SENDS:
            self.copy(mine, mine, 3, self.at(0, dv)).start()

    def start(self):
        mine = self.ref(self.at(0, 0))
        if self.direct:
            for du, dv in FAR_FIRST:
                self.copy(mine, mine, 3, self.at(du, dv)).start()
            return
        for du in SENDS:
            self.copy(mine, mine, STEPS.index(du), self.at(-du, 0)).start()
        self.spread(0)

    def turn(self, du):
        block = self.ref(self.at(du, 0))
        self.copy(block, block, STEPS.index(du), self.at(1, 0)).wait_recv()
        self.spread(du)

    def finish(self):
        many = self.ref(pl.ds(0, PEERS - 1 if self.direct else PEERS - SIDE))
        self.copy(many, many, 3, self.at(1, 0)).wait_recv()

    def drain(self):
        many = self.ref(pl.ds(0, PEERS - 1))
        self.copy(many, many, 3, self.at(1, 0)).wait_send()


def bounds(rows):
    outer, middle = OUTER, MIDDLE
    cuts = []
    for k in range(2 * LAYERS):
        lost = PAD * ((k + 1) // 2)
        cuts.append((0, PAD, outer - lost, middle - lost, rows // 2))
    return cuts


def plan():
    inner = range(1, CHUNKS)
    order = [("turn", c, 0) for c in inner]
    order.insert(2, ("finish", 0, 0))
    last = 2 * LAYERS - 1
    for k in range(last + 1):
        for c in inner:
            order.append(("finish", c, k))
            if k % 2 == 0:
                order.append(("conv", c, k))
                if c == EDGE_AFTER:
                    order.append(("conv", 0, k))
        if k < last:
            order += [("turn", 1, k + 1), ("finish", 0, k + 1)]
            order += [("turn", c, k + 1) for c in inner[1:]]
    return order


def column(row):
    return jnp.swapaxes(jnp.broadcast_to(row, (LANES, LANES)), 0, 1)


def kernel(
    ns,
    stream, doc, wv, wg, ck, cg, cs, wp, og, osh,
    out,
    gbuf, wvg, wpb, ckv, cgv, csv, ogv, osv, docv, docs, nleft, nright, glu, hsend, hrecv, act, keep, z32, stat,
    stsend, strecv,
    load, send, recv, hss, hrs, dss, drs, ss, sr,
):
    rows = stream.shape[0]
    s = lax.axis_index("sp")
    t = lax.axis_index("tp")
    y, x = t // SIDE, t % SIDE
    env = dict(s=s, x=x, y=y, gbuf=gbuf, send=send, recv=recv)
    after, before = lax.rem(s + 1, ns), lax.rem(s + ns - 1, ns)

    loads = [pltpu.make_async_copy(stream, gbuf.at[0, t], load.at[0])]
    loads.append(pltpu.make_async_copy(doc, docv, load.at[1]))
    for n, (src, dst) in enumerate(((ck, ckv), (cg, cgv), (cs, csv), (og, ogv), (osh, osv))):
        loads.append(pltpu.make_async_copy(src, dst, load.at[2 + n]))
    weights = []
    for layer in range(LAYERS):
        weights.append([
            pltpu.make_async_copy(wv.at[layer], wvg.at[layer, :, pl.ds(0, LANES)], load.at[7 + 3 * layer]),
            pltpu.make_async_copy(wg.at[layer], wvg.at[layer, :, pl.ds(LANES, LANES)], load.at[8 + 3 * layer]),
            pltpu.make_async_copy(wp.at[layer], wpb.at[layer], load.at[9 + 3 * layer]),
        ])
    for c in loads:
        c.start()
    for group in weights:
        for c in group:
            c.start()

    barrier = pltpu.get_barrier_semaphore()
    for d in range(1, PEERS):
        pl.semaphore_signal(barrier, inc=1, device_id=(s, lax.rem(t + d, PEERS)), device_id_type=MESH)
    for other in (after, before):
        pl.semaphore_signal(barrier, inc=1, device_id=(other, t), device_id_type=MESH)
    loads[0].wait()
    pl.semaphore_wait(barrier, PEERS + 1)

    cuts = bounds(rows)
    pieces = {}
    for k in range(2 * LAYERS):
        for c in range(CHUNKS):
            low, high = cuts[k][c], cuts[k][c + 1]
            pieces[c, k] = (
                Spread(env, k, 2 * c, low, high - low, True, DIRECT[c]),
                Spread(env, k, 2 * c + 1, rows - high, high - low, False, DIRECT[c]),
            )

    def start(c, k):
        for piece in pieces[c, k]:
            piece.start()

    def halo(src, dst, sem_s, sem_r, who):
        return pltpu.make_async_remote_copy(
            src_ref=src, dst_ref=dst, send_sem=sem_s, recv_sem=sem_r, device_id=(who, t), device_id_type=MESH
        )

    for c in range(CHUNKS):
        start(c, 0)

    loads[1].wait()
    for n in range(rows // LANES):
        docs[PAD + n * LANES : PAD + (n + 1) * LANES, :] = column(
            docv[n * LANES : (n + 1) * LANES].astype(jnp.float32).reshape(1, LANES)
        )
    right_doc = halo(docs.at[pl.ds(rows, PAD)], docs.at[pl.ds(0, PAD)], dss.at[0], drs.at[0], after)
    left_doc = halo(docs.at[pl.ds(PAD, PAD)], docs.at[pl.ds(rows + PAD, PAD)], dss.at[1], drs.at[1], before)
    right_doc.start()
    left_doc.start()
    def prepare():
        for c in loads[2:]:
            c.wait()
        right_doc.wait()
        left_doc.wait()

        @pl.when(s == 0)
        def _():
            docs[0:PAD, :] = jnp.full((PAD, LANES), -1.0, jnp.float32)

        @pl.when(s == ns - 1)
        def _():
            docs[rows + PAD : rows + 2 * PAD, :] = jnp.full((PAD, LANES), -1.0, jnp.float32)

        def reach(n, carry):
            base = pl.multiple_of(n * PAD, PAD)
            mine = docs[pl.ds(base + PAD, PAD), :]
            low = jnp.zeros((PAD, LANES), jnp.float32)
            high = jnp.zeros((PAD, LANES), jnp.float32)
            for j in range(1, HALF + 1):
                low = low + (docs[pl.ds(base + PAD - j, PAD), :] == mine).astype(jnp.float32)
                high = high + (docs[pl.ds(base + PAD + j, PAD), :] == mine).astype(jnp.float32)
            nleft[pl.ds(base, PAD), :] = low
            nright[pl.ds(base, PAD), :] = high
            return carry

        lax.fori_loop(0, rows // PAD, reach, 0)

    def conv_rows(layer, first, last):
        def tile(n, carry):
            base = pl.multiple_of(n * PAD, PAD)
            low = nleft[pl.ds(base, PAD), :]
            high = nright[pl.ds(base, PAD), :]
            taps = ckv[layer].astype(jnp.float32)
            total = glu[layer, pl.ds(base + PAD, PAD), :] * taps[HALF : HALF + 1, :]
            for j in range(1, HALF + 1):
                a = glu[layer, pl.ds(base + PAD - j, PAD), :]
                b = glu[layer, pl.ds(base + PAD + j, PAD), :]
                total = total + jnp.where(low >= j, a, 0.0) * taps[HALF - j : HALF - j + 1, :]
                total = total + jnp.where(high >= j, b, 0.0) * taps[HALF + j : HALF + j + 1, :]
            gbuf[2 * layer + 1, t, pl.ds(base, PAD), :] = total.astype(jnp.bfloat16)
            return carry

        lax.fori_loop(first // PAD, last // PAD, tile, 0)

    def normed(k, layer, gain, shift, silu, part):
        count = part.stop - part.start
        one = jnp.zeros((count, LANES), jnp.float32)
        two = jnp.zeros((count, LANES), jnp.float32)
        for j in range(PEERS):
            v = gbuf[k, j, part, :].astype(jnp.float32)
            one = one + v
            two = two + v * v
        width = PEERS * LANES
        mean = jnp.sum(one, axis=1, keepdims=True) * (1.0 / width)
        var = jnp.maximum(jnp.sum(two, axis=1, keepdims=True) * (1.0 / width) - mean * mean, 0.0)
        scale = lax.rsqrt(var + EPS)
        centre = mean * scale
        for j in range(PEERS):
            v = gbuf[k, j, part, :].astype(jnp.float32)
            cols = slice(j * LANES, (j + 1) * LANES)
            factor, offset = gain[layer : layer + 1, cols], shift[layer : layer + 1, cols]
            if silu:
                factor, offset = 0.5 * factor, 0.5 * offset
            v = (v * scale - centre) * factor + offset
            if silu:
                v = v + v * jnp.tanh(v)
            act[j, part, :] = v.astype(jnp.bfloat16)

    def halos(layer):
        return [
            halo(hsend.at[layer, 1], hrecv.at[layer, 0], hss.at[layer, 0], hrs.at[layer, 0], after),
            halo(hsend.at[layer, 0], hrecv.at[layer, 1], hss.at[layer, 1], hrs.at[layer, 1], before),
        ]

    def sides(c, k):
        return [slice(p.row0, p.row0 + p.rows) for p in pieces[c, k]]

    def joined(ref, parts):
        rows_of = [jnp.concatenate([ref[j, part, :] for j in range(PEERS)], axis=1) for part in parts]
        return jnp.concatenate(rows_of, axis=0)

    pending = {(layer, n) for layer in range(LAYERS) for n in range(2)}

    def loaded(layer, n):
        if (layer, n) in pending:
            pending.remove((layer, n))
            for c in weights[layer][2:] if n else weights[layer][:2]:
                c.wait()

    def gated(c, k):
        layer, parts = k // 2, sides(c, k)
        loaded(layer, 0)
        if layer == 0:
            lhs = joined(gbuf.at[0], parts)
            for part in parts:
                keep[part, :] = gbuf[0, t, part, :].astype(jnp.float32)
        else:
            for part in parts:
                normed(k, layer - 1, ogv, osv, False, part)
                keep[part, :] = act[t, part, :].astype(jnp.float32)
            lhs = joined(act, parts)
        both = jnp.dot(lhs, wvg[layer], preferred_element_type=jnp.float32)
        value = (both[:, :LANES] / (1.0 + jnp.exp(-both[:, LANES:]))).astype(jnp.bfloat16)
        count = pieces[c, k][0].rows
        for n, part in enumerate(parts):
            mine = value[n * count : (n + 1) * count]
            glu[layer, PAD + part.start : PAD + part.stop, :] = mine.astype(jnp.float32)
            if c == 0:
                hsend[layer, n] = mine[:PAD] if n == 0 else mine[count - PAD :]
        if c == 0:
            for h in halos(layer):
                h.start()

    def convolved(c, k):
        layer = k // 2
        left, right = sides(c, k + 1)
        if c == 0:
            for h in halos(layer):
                h.wait()
            glu[layer, 0:PAD, :] = hrecv[layer, 0].astype(jnp.float32)
            glu[layer, rows + PAD : rows + 2 * PAD, :] = hrecv[layer, 1].astype(jnp.float32)
            conv_rows(layer, 0, PAD)
            conv_rows(layer, rows - PAD, rows)
        elif left.stop == right.start:
            conv_rows(layer, left.start, right.stop)
        else:
            conv_rows(layer, left.start, left.stop)
            conv_rows(layer, right.start, right.stop)

    def projected(c, k):
        layer, parts = k // 2, sides(c, k)
        loaded(layer, 1)
        for part in parts:
            normed(k, layer, cgv, csv, True, part)
        branch = jnp.dot(joined(act, parts), wpb[layer], preferred_element_type=jnp.float32)
        count = pieces[c, k][0].rows
        for n, part in enumerate(parts):
            z = ALPHA * keep[part, :] + branch[n * count : (n + 1) * count]
            if layer < LAYERS - 1:
                gbuf[k + 1, t, part, :] = z.astype(jnp.bfloat16)
            else:
                z32[part, :] = z

    order = plan()
    waiting = CHUNKS - sum(DIRECT)
    for what, c, k in order:
        if waiting and what == "turn":
            waiting -= 1
        elif waiting == 0 or (waiting and what == "conv"):
            prepare()
            waiting = None
        if what == "turn":
            for du in STEPS:
                for piece in pieces[c, k]:
                    piece.turn(du)
        elif what == "finish":
            for piece in pieces[c, k]:
                piece.finish()
            if k % 2 == 0:
                gated(c, k)
            else:
                projected(c, k)
                if k + 1 < 2 * LAYERS:
                    start(c, k + 1)
        else:
            convolved(c, k)
            start(c, k + 1)

    ones = jnp.ones((8, LANES), jnp.float32)
    z = z32[...]
    contract = (((1,), (1,)), ((), ()))
    one = lax.dot_general(ones, z, contract, precision=lax.Precision.HIGHEST, preferred_element_type=jnp.float32)
    two = lax.dot_general(ones, z * z, contract, precision=lax.Precision.HIGHEST, preferred_element_type=jnp.float32)
    stsend[0:1, :] = one[0:1, :]
    stsend[1:2, :] = two[0:1, :]
    outgoing = []
    for d in range(1, PEERS):
        c = pltpu.make_async_remote_copy(
            src_ref=stsend,
            dst_ref=strecv.at[d],
            send_sem=ss.at[d],
            recv_sem=sr.at[d],
            device_id=(s, lax.rem(t + d, PEERS)),
            device_id_type=MESH,
        )
        c.start()
        outgoing.append(c)
    sums = stsend[...]
    for d in range(1, PEERS):
        outgoing[d - 1].wait_recv()
        sums = sums + strecv[d]
    stat[...] = sums
    mine = pl.ds(pl.multiple_of(t * LANES, LANES), LANES)
    gain = ogv[LAYERS - 1 : LAYERS, mine]
    shift = osv[LAYERS - 1 : LAYERS, mine]
    width = PEERS * LANES
    for n in range(rows // LANES):
        cols = slice(n * LANES, (n + 1) * LANES)
        mean = column(stat[0:1, cols]) * (1.0 / width)
        var = jnp.maximum(column(stat[1:2, cols]) * (1.0 / width) - mean * mean, 0.0)
        v = (z32[cols, :] - mean) * lax.rsqrt(var + EPS) * gain + shift
        out[cols, :] = v.astype(jnp.bfloat16)
    for c in outgoing:
        c.wait_send()
    for pair in pieces.values():
        for piece in pair:
            piece.drain()


def on_device(ns, stream, doc_ids, w_value, w_gate, conv_kernel, conv_gain, conv_shift, w_proj, out_gain, out_shift):
    rows, width = stream.shape[0], w_value.shape[1]
    gathers = 2 * LAYERS
    bf16, f32 = jnp.bfloat16, jnp.float32
    dma = pltpu.SemaphoreType.DMA
    return pl.pallas_call(
        functools.partial(kernel, ns),
        out_shape=jax.ShapeDtypeStruct((rows, LANES), bf16),
        in_specs=[pl.BlockSpec(memory_space=pl.ANY)] * 10,
        out_specs=pl.BlockSpec(memory_space=pltpu.VMEM),
        scratch_shapes=[
            pltpu.VMEM((gathers, PEERS, rows, LANES), bf16),
            pltpu.VMEM((LAYERS, width, 2 * LANES), bf16),
            pltpu.VMEM((LAYERS, width, LANES), bf16),
            pltpu.VMEM((LAYERS, KERNEL, LANES), bf16),
            pltpu.VMEM((LAYERS, width), f32),
            pltpu.VMEM((LAYERS, width), f32),
            pltpu.VMEM((LAYERS, width), f32),
            pltpu.VMEM((LAYERS, width), f32),
            pltpu.VMEM((rows,), jnp.int32),
            pltpu.VMEM((rows + 2 * PAD, LANES), f32),
            pltpu.VMEM((rows, LANES), f32),
            pltpu.VMEM((rows, LANES), f32),
            pltpu.VMEM((LAYERS, rows + 2 * PAD, LANES), f32),
            pltpu.VMEM((LAYERS, 2, PAD, LANES), bf16),
            pltpu.VMEM((LAYERS, 2, PAD, LANES), bf16),
            pltpu.VMEM((PEERS, rows, LANES), bf16),
            pltpu.VMEM((rows, LANES), f32),
            pltpu.VMEM((rows, LANES), f32),
            pltpu.VMEM((2, rows), f32),
            pltpu.VMEM((2, rows), f32),
            pltpu.VMEM((PEERS, 2, rows), f32),
            dma((7 + 3 * LAYERS,)),
            dma((gathers, 2 * CHUNKS)),
            dma((gathers, 2 * CHUNKS, SIDE)),
            dma((LAYERS, 2)),
            dma((LAYERS, 2)),
            dma((2,)),
            dma((2,)),
            dma((PEERS,)),
            dma((PEERS,)),
        ],
        compiler_params=pltpu.CompilerParams(
            collective_id=0, has_side_effects=True, vmem_limit_bytes=60 * 1024 * 1024
        ),
        name="stack",
    )(stream, doc_ids, w_value, w_gate, conv_kernel, conv_gain, conv_shift, w_proj, out_gain, out_shift)


def solution(mesh):
    return jax.shard_map(
        functools.partial(on_device, mesh.shape["sp"]),
        mesh=mesh,
        in_specs=(
            P("sp", "tp"), P("sp"), P(None, None, "tp"), P(None, None, "tp"), P(None, None, "tp"), P(), P(),
            P(None, None, "tp"), P(), P(),
        ),
        out_specs=P("sp", "tp"),
        check_vma=False,
    )
```

```python
import functools

import jax
import jax.numpy as jnp
from jax import lax
from jax.experimental import pallas as pl
from jax.experimental.pallas import tpu as pltpu
from jax.sharding import PartitionSpec as P

LAYERS = 3
KERNEL = 31
HALF = 15
PAD = 16
LANES = 128
SIDE = 4
PEERS = SIDE * SIDE
STEPS = (1, -1, 2)
SENDS = (2, 1, -1)
FAR_FIRST = [(du, dv) for du in (2, 1, -1, 0) for dv in (2, 1, -1, 0) if (du, dv) != (0, 0)]
CHUNKS = 4
OUTER = 96
MIDDLE = 160
EDGE_AFTER = 1
DIRECT = (True, False, False, False)
ALPHA = 2.0**0.25
EPS = 1e-05
MESH = pl.DeviceIdType.MESH


class Spread:
    def __init__(self, env, stage, piece, row0, rows, x_first, direct):
        self.env, self.k, self.p, self.direct = env, stage, piece, direct
        self.row0, self.rows, self.x_first = row0, rows, x_first

    def at(self, du, dv):
        dx, dy = (du, dv) if self.x_first else (dv, du)
        e = self.env
        return lax.rem(e["y"] + dy + SIDE, SIDE) * SIDE + lax.rem(e["x"] + dx + SIDE, SIDE)

    def ref(self, slot):
        return self.env["gbuf"].at[self.k, slot, pl.ds(self.row0, self.rows), :]

    def copy(self, src, dst, recv, peer):
        e = self.env
        return pltpu.make_async_remote_copy(
            src_ref=src,
            dst_ref=dst,
            send_sem=e["send"].at[self.k, self.p],
            recv_sem=e["recv"].at[self.k, self.p, recv],
            device_id=(e["s"], peer),
            device_id_type=MESH,
        )

    def spread(self, du):
        mine = self.ref(self.at(du, 0))
        for dv in SENDS:
            self.copy(mine, mine, 3, self.at(0, dv)).start()

    def start(self):
        mine = self.ref(self.at(0, 0))
        if self.direct:
            for du, dv in FAR_FIRST:
                self.copy(mine, mine, 3, self.at(du, dv)).start()
            return
        for du in SENDS:
            self.copy(mine, mine, STEPS.index(du), self.at(-du, 0)).start()
        self.spread(0)

    def turn(self, du):
        block = self.ref(self.at(du, 0))
        self.copy(block, block, STEPS.index(du), self.at(1, 0)).wait_recv()
        self.spread(du)

    def finish(self):
        many = self.ref(pl.ds(0, PEERS - 1 if self.direct else PEERS - SIDE))
        self.copy(many, many, 3, self.at(1, 0)).wait_recv()

    def drain(self):
        many = self.ref(pl.ds(0, PEERS - 1))
        self.copy(many, many, 3, self.at(1, 0)).wait_send()


def bounds(rows):
    outer, middle = OUTER, MIDDLE
    cuts = []
    for k in range(2 * LAYERS):
        lost = PAD * ((k + 1) // 2)
        cuts.append((0, PAD, outer - lost, middle - lost, rows // 2))
    return cuts


def plan():
    inner = range(1, CHUNKS)
    order = [("turn", c, 0) for c in inner]
    order.insert(2, ("finish", 0, 0))
    last = 2 * LAYERS - 1
    for k in range(last + 1):
        for c in inner:
            order.append(("finish", c, k))
            if k % 2 == 0:
                order.append(("conv", c, k))
                if c == EDGE_AFTER:
                    order.append(("conv", 0, k))
        if k < last:
            order += [("turn", 1, k + 1), ("finish", 0, k + 1)]
            order += [("turn", c, k + 1) for c in inner[1:]]
    return order


def column(row):
    return jnp.swapaxes(jnp.broadcast_to(row, (LANES, LANES)), 0, 1)


def kernel(
    ns,
    stream, doc, wv, wg, ck, cg, cs, wp, og, osh,
    out,
    gbuf, wvg, wpb, ckv, cgv, csv, ogv, osv, docv, docs, nleft, nright, glu, hsend, hrecv, act, keep, z32, stat,
    stsend, strecv,
    load, send, recv, hss, hrs, dss, drs, ss, sr,
):
    rows = stream.shape[0]
    s = lax.axis_index("sp")
    t = lax.axis_index("tp")
    y, x = t // SIDE, t % SIDE
    env = dict(s=s, x=x, y=y, gbuf=gbuf, send=send, recv=recv)
    after, before = lax.rem(s + 1, ns), lax.rem(s + ns - 1, ns)

    loads = [pltpu.make_async_copy(stream, gbuf.at[0, t], load.at[0])]
    loads.append(pltpu.make_async_copy(doc, docv, load.at[1]))
    for n, (src, dst) in enumerate(((ck, ckv), (cg, cgv), (cs, csv), (og, ogv), (osh, osv))):
        loads.append(pltpu.make_async_copy(src, dst, load.at[2 + n]))
    weights = []
    for layer in range(LAYERS):
        weights.append([
            pltpu.make_async_copy(wv.at[layer], wvg.at[layer, :, pl.ds(0, LANES)], load.at[7 + 3 * layer]),
            pltpu.make_async_copy(wg.at[layer], wvg.at[layer, :, pl.ds(LANES, LANES)], load.at[8 + 3 * layer]),
            pltpu.make_async_copy(wp.at[layer], wpb.at[layer], load.at[9 + 3 * layer]),
        ])
    for c in loads:
        c.start()
    for group in weights:
        for c in group:
            c.start()

    barrier = pltpu.get_barrier_semaphore()
    for d in range(1, PEERS):
        pl.semaphore_signal(barrier, inc=1, device_id=(s, lax.rem(t + d, PEERS)), device_id_type=MESH)
    for other in (after, before):
        pl.semaphore_signal(barrier, inc=1, device_id=(other, t), device_id_type=MESH)
    loads[0].wait()
    pl.semaphore_wait(barrier, PEERS + 1)

    cuts = bounds(rows)
    pieces = {}
    for k in range(2 * LAYERS):
        for c in range(CHUNKS):
            low, high = cuts[k][c], cuts[k][c + 1]
            pieces[c, k] = (
                Spread(env, k, 2 * c, low, high - low, True, DIRECT[c]),
                Spread(env, k, 2 * c + 1, rows - high, high - low, False, DIRECT[c]),
            )

    def start(c, k):
        for piece in pieces[c, k]:
            piece.start()

    def halo(src, dst, sem_s, sem_r, who):
        return pltpu.make_async_remote_copy(
            src_ref=src, dst_ref=dst, send_sem=sem_s, recv_sem=sem_r, device_id=(who, t), device_id_type=MESH
        )

    for c in range(CHUNKS):
        start(c, 0)

    loads[1].wait()
    for n in range(rows // LANES):
        docs[PAD + n * LANES : PAD + (n + 1) * LANES, :] = column(
            docv[n * LANES : (n + 1) * LANES].astype(jnp.float32).reshape(1, LANES)
        )
    right_doc = halo(docs.at[pl.ds(rows, PAD)], docs.at[pl.ds(0, PAD)], dss.at[0], drs.at[0], after)
    left_doc = halo(docs.at[pl.ds(PAD, PAD)], docs.at[pl.ds(rows + PAD, PAD)], dss.at[1], drs.at[1], before)
    right_doc.start()
    left_doc.start()
    def prepare():
        for c in loads[2:]:
            c.wait()
        right_doc.wait()
        left_doc.wait()

        @pl.when(s == 0)
        def _():
            docs[0:PAD, :] = jnp.full((PAD, LANES), -1.0, jnp.float32)

        @pl.when(s == ns - 1)
        def _():
            docs[rows + PAD : rows + 2 * PAD, :] = jnp.full((PAD, LANES), -1.0, jnp.float32)

        def reach(n, carry):
            base = pl.multiple_of(n * PAD, PAD)
            mine = docs[pl.ds(base + PAD, PAD), :]
            low = jnp.zeros((PAD, LANES), jnp.float32)
            high = jnp.zeros((PAD, LANES), jnp.float32)
            for j in range(1, HALF + 1):
                low = low + (docs[pl.ds(base + PAD - j, PAD), :] == mine).astype(jnp.float32)
                high = high + (docs[pl.ds(base + PAD + j, PAD), :] == mine).astype(jnp.float32)
            nleft[pl.ds(base, PAD), :] = low
            nright[pl.ds(base, PAD), :] = high
            return carry

        lax.fori_loop(0, rows // PAD, reach, 0)

    def conv_rows(layer, first, last):
        def tile(n, carry):
            base = pl.multiple_of(n * PAD, PAD)
            low = nleft[pl.ds(base, PAD), :]
            high = nright[pl.ds(base, PAD), :]
            taps = ckv[layer].astype(jnp.float32)
            total = glu[layer, pl.ds(base + PAD, PAD), :] * taps[HALF : HALF + 1, :]
            for j in range(1, HALF + 1):
                a = glu[layer, pl.ds(base + PAD - j, PAD), :]
                b = glu[layer, pl.ds(base + PAD + j, PAD), :]
                total = total + jnp.where(low >= j, a, 0.0) * taps[HALF - j : HALF - j + 1, :]
                total = total + jnp.where(high >= j, b, 0.0) * taps[HALF + j : HALF + j + 1, :]
            gbuf[2 * layer + 1, t, pl.ds(base, PAD), :] = total.astype(jnp.bfloat16)
            return carry

        lax.fori_loop(first // PAD, last // PAD, tile, 0)

    def normed(k, layer, gain, shift, silu, part):
        count = part.stop - part.start
        one = jnp.zeros((count, LANES), jnp.float32)
        two = jnp.zeros((count, LANES), jnp.float32)
        for j in range(PEERS):
            v = gbuf[k, j, part, :].astype(jnp.float32)
            one = one + v
            two = two + v * v
        width = PEERS * LANES
        mean = jnp.sum(one, axis=1, keepdims=True) * (1.0 / width)
        var = jnp.maximum(jnp.sum(two, axis=1, keepdims=True) * (1.0 / width) - mean * mean, 0.0)
        scale = lax.rsqrt(var + EPS)
        centre = mean * scale
        for j in range(PEERS):
            v = gbuf[k, j, part, :].astype(jnp.float32)
            cols = slice(j * LANES, (j + 1) * LANES)
            factor, offset = gain[layer : layer + 1, cols], shift[layer : layer + 1, cols]
            if silu:
                factor, offset = 0.5 * factor, 0.5 * offset
            v = (v * scale - centre) * factor + offset
            if silu:
                v = v + v * jnp.tanh(v)
            act[j, part, :] = v.astype(jnp.bfloat16)

    def halos(layer):
        return [
            halo(hsend.at[layer, 1], hrecv.at[layer, 0], hss.at[layer, 0], hrs.at[layer, 0], after),
            halo(hsend.at[layer, 0], hrecv.at[layer, 1], hss.at[layer, 1], hrs.at[layer, 1], before),
        ]

    def sides(c, k):
        return [slice(p.row0, p.row0 + p.rows) for p in pieces[c, k]]

    def joined(ref, parts):
        rows_of = [jnp.concatenate([ref[j, part, :] for j in range(PEERS)], axis=1) for part in parts]
        return jnp.concatenate(rows_of, axis=0)

    pending = {(layer, n) for layer in range(LAYERS) for n in range(2)}

    def loaded(layer, n):
        if (layer, n) in pending:
            pending.remove((layer, n))
            for c in weights[layer][2:] if n else weights[layer][:2]:
                c.wait()

    def gated(c, k):
        layer, parts = k // 2, sides(c, k)
        loaded(layer, 0)
        if layer == 0:
            lhs = joined(gbuf.at[0], parts)
            for part in parts:
                keep[part, :] = gbuf[0, t, part, :].astype(jnp.float32)
        else:
            for part in parts:
                normed(k, layer - 1, ogv, osv, False, part)
                keep[part, :] = act[t, part, :].astype(jnp.float32)
            lhs = joined(act, parts)
        both = jnp.dot(lhs, wvg[layer], preferred_element_type=jnp.float32)
        half_lin = 0.5 * both[:, :LANES]
        value = (half_lin + half_lin * jnp.tanh(0.5 * both[:, LANES:])).astype(jnp.bfloat16)
        count = pieces[c, k][0].rows
        for n, part in enumerate(parts):
            mine = value[n * count : (n + 1) * count]
            glu[layer, PAD + part.start : PAD + part.stop, :] = mine.astype(jnp.float32)
            if c == 0:
                hsend[layer, n] = mine[:PAD] if n == 0 else mine[count - PAD :]
        if c == 0:
            for h in halos(layer):
                h.start()

    def convolved(c, k):
        layer = k // 2
        left, right = sides(c, k + 1)
        if c == 0:
            for h in halos(layer):
                h.wait()
            glu[layer, 0:PAD, :] = hrecv[layer, 0].astype(jnp.float32)
            glu[layer, rows + PAD : rows + 2 * PAD, :] = hrecv[layer, 1].astype(jnp.float32)
            conv_rows(layer, 0, PAD)
            conv_rows(layer, rows - PAD, rows)
        elif left.stop == right.start:
            conv_rows(layer, left.start, right.stop)
        else:
            conv_rows(layer, left.start, left.stop)
            conv_rows(layer, right.start, right.stop)

    def projected(c, k):
        layer, parts = k // 2, sides(c, k)
        loaded(layer, 1)
        for part in parts:
            normed(k, layer, cgv, csv, True, part)
        branch = jnp.dot(joined(act, parts), wpb[layer], preferred_element_type=jnp.float32)
        count = pieces[c, k][0].rows
        for n, part in enumerate(parts):
            z = ALPHA * keep[part, :] + branch[n * count : (n + 1) * count]
            if layer < LAYERS - 1:
                gbuf[k + 1, t, part, :] = z.astype(jnp.bfloat16)
            else:
                z32[part, :] = z

    order = plan()
    waiting = CHUNKS - sum(DIRECT)
    for what, c, k in order:
        if waiting and what == "turn":
            waiting -= 1
        elif waiting == 0 or (waiting and what == "conv"):
            prepare()
            waiting = None
        if what == "turn":
            for du in STEPS:
                for piece in pieces[c, k]:
                    piece.turn(du)
        elif what == "finish":
            for piece in pieces[c, k]:
                piece.finish()
            if k % 2 == 0:
                gated(c, k)
            else:
                projected(c, k)
                if k + 1 < 2 * LAYERS:
                    start(c, k + 1)
        else:
            convolved(c, k)
            start(c, k + 1)

    ones = jnp.ones((8, LANES), jnp.float32)
    z = z32[...]
    contract = (((1,), (1,)), ((), ()))
    one = lax.dot_general(ones, z, contract, precision=lax.Precision.HIGHEST, preferred_element_type=jnp.float32)
    two = lax.dot_general(ones, z * z, contract, precision=lax.Precision.HIGHEST, preferred_element_type=jnp.float32)
    stsend[0:1, :] = one[0:1, :]
    stsend[1:2, :] = two[0:1, :]
    outgoing = []
    peers = sorted(range(1, PEERS), key=lambda d: abs(d - PEERS // 2 - 2))
    for d in peers:
        c = pltpu.make_async_remote_copy(
            src_ref=stsend,
            dst_ref=strecv.at[d],
            send_sem=ss.at[d],
            recv_sem=sr.at[d],
            device_id=(s, lax.rem(t + d, PEERS)),
            device_id_type=MESH,
        )
        c.start()
        outgoing.append(c)
    sums = stsend[...]
    for n, d in enumerate(peers):
        outgoing[n].wait_recv()
        sums = sums + strecv[d]
    stat[...] = sums
    mine = pl.ds(pl.multiple_of(t * LANES, LANES), LANES)
    gain = ogv[LAYERS - 1 : LAYERS, mine]
    shift = osv[LAYERS - 1 : LAYERS, mine]
    width = PEERS * LANES
    for n in range(rows // LANES):
        cols = slice(n * LANES, (n + 1) * LANES)
        mean = column(stat[0:1, cols]) * (1.0 / width)
        var = jnp.maximum(column(stat[1:2, cols]) * (1.0 / width) - mean * mean, 0.0)
        v = (z32[cols, :] - mean) * lax.rsqrt(var + EPS) * gain + shift
        out[cols, :] = v.astype(jnp.bfloat16)
    for c in outgoing:
        c.wait_send()
    for pair in pieces.values():
        for piece in pair:
            piece.drain()


def on_device(ns, stream, doc_ids, w_value, w_gate, conv_kernel, conv_gain, conv_shift, w_proj, out_gain, out_shift):
    rows, width = stream.shape[0], w_value.shape[1]
    gathers = 2 * LAYERS
    bf16, f32 = jnp.bfloat16, jnp.float32
    dma = pltpu.SemaphoreType.DMA
    return pl.pallas_call(
        functools.partial(kernel, ns),
        out_shape=jax.ShapeDtypeStruct((rows, LANES), bf16),
        in_specs=[pl.BlockSpec(memory_space=pl.ANY)] * 10,
        out_specs=pl.BlockSpec(memory_space=pltpu.VMEM),
        scratch_shapes=[
            pltpu.VMEM((gathers, PEERS, rows, LANES), bf16),
            pltpu.VMEM((LAYERS, width, 2 * LANES), bf16),
            pltpu.VMEM((LAYERS, width, LANES), bf16),
            pltpu.VMEM((LAYERS, KERNEL, LANES), bf16),
            pltpu.VMEM((LAYERS, width), f32),
            pltpu.VMEM((LAYERS, width), f32),
            pltpu.VMEM((LAYERS, width), f32),
            pltpu.VMEM((LAYERS, width), f32),
            pltpu.VMEM((rows,), jnp.int32),
            pltpu.VMEM((rows + 2 * PAD, LANES), f32),
            pltpu.VMEM((rows, LANES), f32),
            pltpu.VMEM((rows, LANES), f32),
            pltpu.VMEM((LAYERS, rows + 2 * PAD, LANES), f32),
            pltpu.VMEM((LAYERS, 2, PAD, LANES), bf16),
            pltpu.VMEM((LAYERS, 2, PAD, LANES), bf16),
            pltpu.VMEM((PEERS, rows, LANES), bf16),
            pltpu.VMEM((rows, LANES), f32),
            pltpu.VMEM((rows, LANES), f32),
            pltpu.VMEM((2, rows), f32),
            pltpu.VMEM((2, rows), f32),
            pltpu.VMEM((PEERS, 2, rows), f32),
            dma((7 + 3 * LAYERS,)),
            dma((gathers, 2 * CHUNKS)),
            dma((gathers, 2 * CHUNKS, SIDE)),
            dma((LAYERS, 2)),
            dma((LAYERS, 2)),
            dma((2,)),
            dma((2,)),
            dma((PEERS,)),
            dma((PEERS,)),
        ],
        compiler_params=pltpu.CompilerParams(
            collective_id=0, has_side_effects=True, vmem_limit_bytes=60 * 1024 * 1024
        ),
        name="stack",
    )(stream, doc_ids, w_value, w_gate, conv_kernel, conv_gain, conv_shift, w_proj, out_gain, out_shift)


def solution(mesh):
    return jax.shard_map(
        functools.partial(on_device, mesh.shape["sp"]),
        mesh=mesh,
        in_specs=(
            P("sp", "tp"), P("sp"), P(None, None, "tp"), P(None, None, "tp"), P(None, None, "tp"), P(), P(),
            P(None, None, "tp"), P(), P(),
        ),
        out_specs=P("sp", "tp"),
        check_vma=False,
    )
```
